512 devices in a mesh: sp: 32 (over z, x), dp: 16 (over y, core).
Axes of the slice: x: 4, y: 8, z: 8, core: 2. Of those that a mesh axis runs over, the one named last changes fastest.
Arguments:
- query_rows: bfloat16 [16, 4096, 2048], P('dp', 'sp'), may hold values from -6 to 6
- key_rows: bfloat16 [16, 4096, 2048], P('dp', 'sp'), may hold values from -6 to 6
- value_rows: bfloat16 [16, 4096, 2048], P('dp', 'sp'), may hold values from -6 to 6
- decay_low: bfloat16 [16, 4096, 128], P('dp', 'sp'), may hold values from -5 to 5
- rate_low: bfloat16 [16, 4096, 128], P('dp', 'sp'), may hold values from -4 to 4
- decay_up: bfloat16 [128, 2048], replicated, may hold values from -0.5 to 0.5
- rate_up: bfloat16 [128, 2048], replicated, may hold values from -0.5 to 0.5
- decay_base: float32 [2048], replicated, may hold values from -12 to -2
- norm_gain: float32 [2048], replicated, may hold values from 0.1 to 1.9
- out_weight: bfloat16 [2048, 2048], P(None, 'dp'), may hold values from -0.125 to 0.125
Outputs:
- layer_out: bfloat16 [16, 4096, 2048], P('dp', 'sp')
The draws below stay inside these ranges and needn't reach their ends.
All inputs are finite; a program needn't handle non-finite values.
Results may differ from the reference program's by a relative error of at most 0.005.
Values may be sent and summed in bfloat16 or wider, within the bound.
A program may use at most 128 MiB of HBM per device.

```python
import jax
import jax.numpy as jnp
from jax import lax

D = 2048
HEADS = 32
HEAD = 64
LOW = 128
TOK_DEV = 128
WIDTH = 2048
LENGTH = 4096
BATCH = 16


def draw_decay_low(key, part):
    noise = jnp.clip(jax.random.normal(jax.random.fold_in(key, 11), (BATCH, LENGTH, LOW), jnp.float32), -4.0, 4.0)
    offsets = jax.random.uniform(jax.random.fold_in(key, 12), (BATCH, LENGTH // TOK_DEV, 1), jnp.float32, minval=-1.0, maxval=1.0)
    total = noise + jnp.repeat(offsets, TOK_DEV, axis=1)
    return jnp.clip(total, -5.0, 5.0).astype(jnp.bfloat16)


def draw_decay_base(key, part):
    picks = jax.random.randint(jax.random.fold_in(key, 21), (HEADS, 1), 0, 16)
    quick = picks < 8
    slow_rate = jax.random.uniform(jax.random.fold_in(key, 22), (HEADS, HEAD), jnp.float32, minval=0.2, maxval=1.0) / LENGTH
    quick_rate = jax.random.uniform(jax.random.fold_in(key, 23), (HEADS, HEAD), jnp.float32, minval=0.01, maxval=0.033)
    chosen = jnp.where(quick, quick_rate, slow_rate)
    return jnp.clip(jnp.log(chosen) + 0.5, -12.0, -2.0).reshape(WIDTH).astype(jnp.float32)


def block_levels(key, extent, pieces, least, top_value):
    level = 1.0
    for dim, parts in pieces:
        heights = jax.random.uniform(jax.random.fold_in(jax.random.fold_in(key, 6), dim), (parts,), jnp.float32, least / len(pieces), top_value / len(pieces))
        level = level * jnp.repeat(jnp.exp(heights), extent[dim] // parts).reshape((-1,) + (1,) * (len(extent) - 1 - dim))
    return level


def gaussian(stream_key, dims, deviation, reach, cuts=(), held_as=jnp.bfloat16):
    values = deviation * jax.random.normal(stream_key, dims, jnp.float32)
    if cuts:
        values = values * block_levels(stream_key, dims, cuts, -0.22, 0.18)
    return jnp.clip(values, -reach, reach).astype(held_as)


def setup_inputs(seed: int = 0) -> dict:
    splits = jax.random.split(jax.random.key(seed), 11)
    query_rows = gaussian(splits[0], (BATCH, LENGTH, WIDTH), 1.0, 6.0, ((0, 16), (1, 32)))
    key_rows = gaussian(splits[1], (BATCH, LENGTH, WIDTH), 1.0, 6.0, ((0, 16), (1, 32)))
    value_rows = gaussian(splits[2], (BATCH, LENGTH, WIDTH), 1.0, 6.0, ((0, 16), (1, 32)))
    decay_low = draw_decay_low(jax.random.fold_in(splits[10], 71), 0)
    rate_low = gaussian(splits[4], (BATCH, LENGTH, LOW), 1.0, 4.0, ((0, 16), (1, 32)))
    decay_up = gaussian(splits[5], (LOW, WIDTH), LOW ** -0.5, 0.5)
    rate_up = gaussian(splits[6], (LOW, WIDTH), LOW ** -0.5, 0.5)
    decay_base = draw_decay_base(jax.random.fold_in(splits[10], 71), 0)
    norm_gain = jnp.clip(1.0 + 0.18 * jax.random.normal(splits[8], (WIDTH,), jnp.float32), 0.1, 1.9)
    out_weight = gaussian(splits[9], (WIDTH, D), WIDTH ** -0.5, 0.125, ((1, 16),))
    return {"query_rows": query_rows, "key_rows": key_rows, "value_rows": value_rows, "decay_low": decay_low, "rate_low": rate_low, "decay_up": decay_up, "rate_up": rate_up, "decay_base": decay_base, "norm_gain": norm_gain, "out_weight": out_weight}


HIGHEST = lax.Precision.HIGHEST

def reference(query_rows, key_rows, value_rows, decay_low, rate_low, decay_up, rate_up, decay_base, norm_gain, out_weight):
    heads = query_rows.shape[2] // HEAD

    def one_sequence(inputs):
        reads, keyed, valued, low_decay, low_rate = inputs
        positions = reads.shape[0]
        squashed = jnp.tanh(low_decay.astype(jnp.float32)).astype(jnp.bfloat16)
        decay_pre = (decay_base + jnp.dot(squashed, decay_up, preferred_element_type=jnp.float32)).astype(jnp.bfloat16)
        rate_pre = jnp.dot(low_rate, rate_up, preferred_element_type=jnp.float32).astype(jnp.bfloat16)
        log_decay = -jnp.exp(-jax.nn.softplus(-decay_pre.astype(jnp.float32)) - 0.5)
        rate = jax.nn.sigmoid(rate_pre.astype(jnp.float32))
        head_shape = (positions, heads, HEAD)
        query_heads = reads.astype(jnp.float32).reshape(head_shape)
        key_heads = keyed.astype(jnp.float32).reshape(head_shape)
        value_heads = valued.astype(jnp.float32).reshape(head_shape)
        decay_heads = jnp.exp(log_decay).reshape(head_shape)
        unit_keys = key_heads * lax.rsqrt(1.0 + lax.optimization_barrier(jnp.sum(key_heads * key_heads, axis=-1, keepdims=True)))
        erase = unit_keys * rate.reshape(head_shape)

        def advance(state, inputs_now):
            query_now, decay_now, key_now, value_now, unit_now, erase_now = inputs_now
            removed = jnp.einsum('hvk,hk->hv', state, unit_now, precision=HIGHEST)
            state = state * decay_now[:, None, :] - removed[:, :, None] * erase_now[:, None, :] + value_now[:, :, None] * key_now[:, None, :]
            return (state, jnp.einsum('hvk,hk->hv', state, query_now, precision=HIGHEST))
        initial = jnp.zeros((heads, HEAD, HEAD), jnp.float32)
        _, readout = lax.scan(advance, initial, (query_heads, decay_heads, key_heads, value_heads, unit_keys, erase))
        average = lax.optimization_barrier(jnp.mean(readout, axis=-1, keepdims=True))
        centred = readout - average
        variance = lax.optimization_barrier(jnp.mean(centred * centred, axis=-1, keepdims=True))
        normed = (centred * lax.rsqrt(variance + 1.0)).reshape(positions, heads * HEAD)
        mix = (normed * norm_gain).astype(jnp.bfloat16)
        return jnp.dot(mix, out_weight, preferred_element_type=jnp.float32).astype(jnp.bfloat16)
    return lax.map(one_sequence, (query_rows, key_rows, value_rows, decay_low, rate_low))
```

```python
import math

import jax
import jax.numpy as jnp
from jax import lax
from jax.experimental import pallas as pl
from jax.experimental.pallas import tpu as pltpu
from jax.sharding import PartitionSpec as P

HEAD = 64
L = 128
F32 = jnp.float32
BF16 = jnp.bfloat16
MSG = 80


def split(x):
    high = x.astype(BF16)
    return high, (x - high.astype(F32)).astype(BF16)


def mm(a, b):
    return jnp.dot(a, b, preferred_element_type=F32)


def mm_t(a, b):
    return lax.dot_general(a, b, (((1,), (1,)), ((), ())), preferred_element_type=F32)


def t_mm(a, b):
    return lax.dot_general(a, b, (((0,), (0,)), ((), ())), preferred_element_type=F32)


def cols(*parts):
    return jnp.concatenate(parts, axis=1)


def rows(*parts):
    return jnp.concatenate(parts, axis=0)


def grid_index(n=L):
    return (
        lax.broadcasted_iota(jnp.int32, (n, n), 0),
        lax.broadcasted_iota(jnp.int32, (n, n), 1),
    )


def half_masks(dtype, width=L):
    lane = lax.broadcasted_iota(jnp.int32, (1, width), 1) % L
    return (lane < HEAD).astype(dtype), (lane >= HEAD).astype(dtype)


def prepare(pair, refs, s):
    lanes = pl.ds(pl.multiple_of(pair * L, L), L)
    row, col = grid_index()
    first, second = half_masks(BF16)
    decay_pre = (
        refs["base"][:, lanes] + mm(refs["squashed"][...], refs["decay_up"][:, lanes])
    ).astype(BF16)
    rate_pre = mm(refs["rate_low"][...], refs["rate_up"][:, lanes]).astype(BF16)
    log_decay = -math.exp(-0.5) / (1.0 + jnp.exp(-decay_pre.astype(F32)))
    rate = 1.0 / (1.0 + jnp.exp(-rate_pre.astype(F32)))
    tri = (row >= col).astype(BF16)
    running = mm(cols(tri, tri), rows(*split(log_decay)))
    before = running - log_decay
    centre = running[L // 2 : L // 2 + 1]
    final = running[L - 1 : L]
    key = refs["key"][:, lanes].astype(F32)
    query = refs["query"][:, lanes].astype(F32)
    block = (row // HEAD == col // HEAD).astype(BF16)
    total = mm(cols(*split(key * key)), rows(block, block))
    unit = key * lax.rsqrt(1.0 + total)
    erase = unit * rate
    grown = jnp.exp(running - centre)
    shrunk = jnp.exp(centre - running)
    read_mid = query * grown
    erase_from = unit * jnp.exp(before - centre)
    key_to = key * shrunk
    erase_to = erase * shrunk
    up = jnp.exp(centre)
    down = jnp.exp(final - centre)
    s["read_start"][:, lanes] = read_mid * up
    s["erase_start"][:, lanes] = erase_from * up
    s["key_end"][:, lanes] = key_to * down
    s["erase_end"][:, lanes] = erase_to * down
    s["decay"][:, lanes] = jnp.exp(final)
    from_high, from_low = split(rows(erase_from, read_mid))
    left = cols(from_high, from_low)
    strict = row > col
    within = row >= col
    key_high, key_low = split(key_to)
    erase_high, erase_low = split(erase_to)
    for h, mask in enumerate((first, second)):
        head = 2 * pair + h
        a, b = key_high * mask, key_low * mask
        out = mm_t(left, rows(cols(a, a), cols(b, b)))
        out = out[:, :L] + out[:, L:]
        high, low = split(
            rows(jnp.where(strict, out[:L], 0.0), jnp.where(within, out[L:], 0.0))
        )
        s["on_values"][pair, :, h * L : h * L + L] = high
        s["on_values"][pair, :, (2 + h) * L : (3 + h) * L] = low
        a, b = erase_high * mask, erase_low * mask
        out = mm_t(left, rows(cols(a, a), cols(b, b)))
        out = out[:, :L] + out[:, L:]
        high, low = split(jnp.where(within, out[L:], 0.0))
        s["read_erase"][pair, :, h * L : h * L + L] = high
        s["read_erase"][pair, :, (2 + h) * L : (3 + h) * L] = low
        pairs = jnp.where(strict, out[:L], 0.0)
        high, low = split(pairs)
        s["lower"][head, :, :L] = high
        s["lower"][head, :, L:] = low
        next_to = (row // 2 == col // 2) & (row != col)
        s["inverse"][head] = (row == col).astype(F32) - jnp.where(next_to, pairs, 0.0)


def times(left, right):
    a, b = split(right)
    row = cols(a, b)
    out = mm(left, rows(row, row))
    return out[:, :L] + out[:, L:]


def refine(head0, count, level, s):
    row, col = grid_index()
    mask = ((row >> (level + 1)) == (col >> (level + 1))) & ((row >> level) != (col >> level))
    mask = mask.astype(BF16)
    mask = cols(mask, mask)
    held = [s["inverse"][head0 + i] for i in range(count)]
    below = [times(s["lower"][head0 + i] * mask, held[i]) for i in range(count)]
    for i in range(count):
        s["inverse"][head0 + i] = held[i] - times(cols(*split(held[i])), below[i])


def finish(pair, refs, s, out):
    lanes = pl.ds(pl.multiple_of(pair * L, L), L)
    first, second = half_masks(BF16)
    first2, second2 = half_masks(BF16, 2 * L)
    value = refs["value"][:, lanes]
    both = rows(value * first, value * second)
    seen = mm(s["on_values"][pair], rows(both, both))
    carried, local = seen[:L], seen[L:]

    def on_pair(left, right):
        high, low = split(right)
        high = rows(high * first2, high * second2)
        low = rows(low * first2, low * second2)
        return mm(left, rows(high, high)) + mm(left[:, : 2 * L], low)

    d0, d1 = split(s["inverse"][2 * pair]), split(s["inverse"][2 * pair + 1])
    solved = on_pair(
        cols(d0[0], d1[0], d0[1], d1[1]), cols(s["erase_start"][:, lanes], carried)
    )
    on_erase = on_pair(s["read_erase"][pair], solved)
    out["read_state"][:, lanes] = s["read_start"][:, lanes] - on_erase[:, :L]
    out["local"][:, lanes] = local - on_erase[:, L:]
    weights, taken = solved[:, :L], solved[:, L:]
    kh, kl = split(s["key_end"][:, lanes])
    eh, el = split(s["erase_end"][:, lanes])
    wh, wl = split(weights)
    th, tl = split(-taken)
    added = t_mm(rows(value, value, th, tl, th), rows(kh, kl, eh, eh, el))
    moved = t_mm(rows(wh, wl, wh), rows(eh, eh, el))
    decay = jnp.broadcast_to(s["decay"][:, lanes], (16, L))
    dh = decay.astype(BF16).astype(F32)
    dl = decay - dh
    low_half = lax.broadcasted_iota(jnp.int32, (HEAD, L), 1) < HEAD
    turn = lambda x: pltpu.roll(x, HEAD, 1)
    out["message"][2 * pair, :HEAD] = jnp.where(
        low_half, added[:HEAD], turn(moved[:HEAD])
    ).astype(BF16)
    out["message"][2 * pair, HEAD:] = jnp.where(low_half[:16], dh, turn(dl)).astype(BF16)
    out["message"][2 * pair + 1, :HEAD] = jnp.where(
        low_half, turn(added[HEAD:]), moved[HEAD:]
    ).astype(BF16)
    out["message"][2 * pair + 1, HEAD:] = jnp.where(low_half[:16], turn(dh), dl).astype(BF16)


LOCAL_IN = (
    "query",
    "key",
    "value",
    "decay_low",
    "rate_low",
    "decay_up",
    "rate_up",
    "base",
)
LOCAL_OUT = ("read_state", "local", "message")


def local_scratch(width):
    pairs = width // L
    wide = lambda: pltpu.VMEM((L, width), F32)
    return dict(
        squashed=pltpu.VMEM((L, L), BF16),
        read_start=wide(),
        erase_start=wide(),
        key_end=wide(),
        erase_end=wide(),
        decay=pltpu.VMEM((1, width), F32),
        on_values=pltpu.VMEM((pairs, 2 * L, 4 * L), BF16),
        read_erase=pltpu.VMEM((pairs, L, 4 * L), BF16),
        lower=pltpu.VMEM((2 * pairs, L, 2 * L), BF16),
        inverse=pltpu.VMEM((2 * pairs, L, L), F32),
    )


def local_phases(refs, s, out, width, group=(2, 8, 2)):
    pairs = width // L
    s["squashed"][...] = jnp.tanh(refs["decay_low"][...].astype(F32)).astype(BF16)
    refs = dict(refs, squashed=s["squashed"])

    @pl.loop(0, pairs // group[0])
    def _(i):
        for j in range(group[0]):
            prepare(i * group[0] + j, refs, s)

    for level in range(1, 7):

        @pl.loop(0, 2 * pairs // group[1])
        def _(i):
            refine(i * group[1], group[1], level, s)

    @pl.loop(0, pairs // group[2])
    def _(i):
        for j in range(group[2]):
            finish(i * group[2] + j, refs, s, out)


def local_kernel(*args, width):
    n_in, n_out = len(LOCAL_IN), len(LOCAL_OUT)
    refs = dict(zip(LOCAL_IN, args[:n_in]))
    out = dict(zip(LOCAL_OUT, args[n_in : n_in + n_out]))
    s = dict(zip(local_scratch(width), args[n_in + n_out :]))
    local_phases(refs, s, out, width)


def run_local(*args):
    width = args[0].shape[1]
    heads = width // HEAD
    vmem = pl.BlockSpec(memory_space=pltpu.VMEM)
    return pl.pallas_call(
        lambda *a: local_kernel(*a, width=width),
        out_shape=(
            jax.ShapeDtypeStruct((L, width), F32),
            jax.ShapeDtypeStruct((L, width), F32),
            jax.ShapeDtypeStruct((heads, MSG, L), BF16),
        ),
        in_specs=[vmem] * len(LOCAL_IN),
        out_specs=(vmem,) * 3,
        scratch_shapes=list(local_scratch(width).values()),
        compiler_params=pltpu.CompilerParams(vmem_limit_bytes=60 * 2**20),
        name="local",
    )(*args)


def scan_kernel(message, states, added, moved, decay):
    count = message.shape[0]
    low_half = lax.broadcasted_iota(jnp.int32, (HEAD, L), 1) < HEAD
    turn = lambda x: pltpu.roll(x, HEAD, 1)

    @pl.loop(0, count)
    def _(n):
        both = message[n, :HEAD].astype(F32)
        added[n] = both
        moved[n] = jnp.where(low_half, turn(both), 0.0).astype(BF16)
        parts = message[n, HEAD:].astype(F32)
        decay[n] = (parts + turn(parts))[:8]

    def step(n, state):
        high, low = split(state)
        states[n] = jnp.where(
            low_half[: HEAD // 2], state[: HEAD // 2], turn(state[HEAD // 2 :])
        ).astype(BF16)
        out = mm(rows(high, low)[:, :HEAD], moved[n])
        state = state * decay[n][:1] - (out[:HEAD] + out[HEAD:]) + added[n]
        return state

    lax.fori_loop(0, count, step, jnp.zeros((HEAD, L), F32))


def run_scan(message):
    count = message.shape[0]
    vmem = pl.BlockSpec(memory_space=pltpu.VMEM)
    return pl.pallas_call(
        scan_kernel,
        out_shape=jax.ShapeDtypeStruct((count, HEAD // 2, L), BF16),
        in_specs=[vmem],
        out_specs=vmem,
        scratch_shapes=[
            pltpu.VMEM((count, HEAD, L), F32),
            pltpu.VMEM((count, HEAD, L), BF16),
            pltpu.VMEM((count, 8, L), F32),
        ],
        name="scan",
    )(message)


def read_pair(pair, read_state, local, states, gain, mix):
    lanes = pl.ds(pl.multiple_of(pair * L, L), L)
    low_half = lax.broadcasted_iota(jnp.int32, (HEAD // 2, L), 1) < HEAD
    turn = lambda x: pltpu.roll(x, HEAD, 1)
    a = states[2 * pair].astype(F32)
    b = states[2 * pair + 1].astype(F32)
    state = rows(
        jnp.where(low_half, a, 0.0),
        jnp.where(low_half, turn(a), 0.0),
        jnp.where(low_half, 0.0, turn(b)),
        jnp.where(low_half, 0.0, b),
    ).astype(BF16)
    readout = mm_t(cols(*split(read_state[:, lanes])), cols(state, state)) + local[:, lanes]
    row, col = grid_index()
    block = (row // HEAD == col // HEAD).astype(BF16)
    block = rows(block, block)
    centred = readout - mm(cols(*split(readout)), block) * (1.0 / HEAD)
    variance = mm(cols(*split(centred * centred)), block) * (1.0 / HEAD)
    mix[:, lanes] = (centred * lax.rsqrt(variance + 1.0) * gain[:, lanes]).astype(BF16)


def output_kernel(read_state, local, states, gain, weight, out, mix):
    pairs = read_state.shape[1] // L

    @pl.loop(0, pairs // 4)
    def _(i):
        for j in range(4):
            read_pair(i * 4 + j, read_state, local, states, gain, mix)

    @pl.loop(0, weight.shape[0] // 2)
    def _(i):
        both = cols(weight[2 * i], weight[2 * i + 1])
        out[:, pl.ds(pl.multiple_of(i * 2 * L, 2 * L), 2 * L)] = mm(mix[...], both).astype(BF16)


def run_output(read_state, local, states, gain, weight):
    vmem = pl.BlockSpec(memory_space=pltpu.VMEM)
    return pl.pallas_call(
        output_kernel,
        out_shape=jax.ShapeDtypeStruct((L, weight.shape[0] * weight.shape[2]), BF16),
        in_specs=[vmem] * 5,
        out_specs=vmem,
        scratch_shapes=[pltpu.VMEM(read_state.shape, BF16)],
        compiler_params=pltpu.CompilerParams(vmem_limit_bytes=60 * 2**20),
        name="output",
    )(read_state, local, states, gain, weight)


def per_device(
    query_rows, key_rows, value_rows, decay_low, rate_low, decay_up, rate_up, decay_base, norm_gain, out_weight
):
    weight = lax.all_gather(out_weight, "dp")
    read_state, local, message = run_local(
        query_rows[0], key_rows[0], value_rows[0], decay_low[0], rate_low[0],
        decay_up, rate_up, decay_base[None],
    )
    got = lax.all_to_all(message, "sp", split_axis=0, concat_axis=0, tiled=True)
    states = run_scan(got)
    starts = lax.all_to_all(states, "sp", split_axis=0, concat_axis=0, tiled=True)
    return run_output(read_state, local, starts, norm_gain[None], weight)[None]


def solution(mesh):
    rows_spec = P("dp", "sp", None)
    return jax.shard_map(
        per_device,
        mesh=mesh,
        in_specs=(rows_spec,) * 5 + (P(), P(), P(), P(), P(None, "dp")),
        out_specs=rows_spec,
        check_vma=False,
    )
```

```python
import functools
import math

import jax
import jax.numpy as jnp
from jax import lax
from jax.experimental import pallas as pl
from jax.experimental.pallas import tpu as pltpu
from jax.sharding import PartitionSpec as P

HEAD = 64
L = 128
F32 = jnp.float32
BF16 = jnp.bfloat16
MSG = 80


def split(x):
    high = x.astype(BF16)
    return high, (x - high.astype(F32)).astype(BF16)


def mm(a, b):
    return jnp.dot(a, b, preferred_element_type=F32)


def mm_t(a, b):
    return lax.dot_general(a, b, (((1,), (1,)), ((), ())), preferred_element_type=F32)


def t_mm(a, b):
    return lax.dot_general(a, b, (((0,), (0,)), ((), ())), preferred_element_type=F32)


def cols(*parts):
    return jnp.concatenate(parts, axis=1)


def rows(*parts):
    return jnp.concatenate(parts, axis=0)


def grid_index(n=L):
    return (
        lax.broadcasted_iota(jnp.int32, (n, n), 0),
        lax.broadcasted_iota(jnp.int32, (n, n), 1),
    )


def half_masks(dtype, width=L):
    lane = lax.broadcasted_iota(jnp.int32, (1, width), 1) % L
    return (lane < HEAD).astype(dtype), (lane >= HEAD).astype(dtype)


def prepare(pair, refs, s):
    lanes = pl.ds(pl.multiple_of(pair * L, L), L)
    row, col = grid_index()
    first, second = half_masks(BF16)
    decay_pre = (
        refs["base"][:, lanes] + mm(refs["squashed"][...], refs["decay_up"][:, lanes])
    ).astype(BF16)
    rate_pre = mm(refs["rate_low"][...], refs["rate_up"][:, lanes]).astype(BF16)
    log_decay = -math.exp(-0.5) / (1.0 + jnp.exp(-decay_pre.astype(F32)))
    rate = 1.0 / (1.0 + jnp.exp(-rate_pre.astype(F32)))
    tri = (row >= col).astype(BF16)
    running = mm(cols(tri, tri), rows(*split(log_decay)))
    before = running - log_decay
    centre = running[L // 2 : L // 2 + 1]
    final = running[L - 1 : L]
    key = refs["key"][:, lanes].astype(F32)
    query = refs["query"][:, lanes].astype(F32)
    block = (row // HEAD == col // HEAD).astype(BF16)
    total = mm(cols(*split(key * key)), rows(block, block))
    unit = key * lax.rsqrt(1.0 + total)
    erase = unit * rate
    grown = jnp.exp(running - centre)
    shrunk = jnp.exp(centre - running)
    read_mid = query * grown
    erase_from = unit * jnp.exp(before - centre)
    key_to = key * shrunk
    erase_to = erase * shrunk
    up = jnp.exp(centre)
    down = jnp.exp(final - centre)
    s["read_start"][:, lanes] = read_mid * up
    s["erase_start"][:, lanes] = erase_from * up
    s["key_end"][:, lanes] = key_to * down
    s["erase_end"][:, lanes] = erase_to * down
    s["decay"][:, lanes] = jnp.exp(final)
    from_high, from_low = split(rows(erase_from, read_mid))
    left = cols(from_high, from_low)
    strict = row > col
    within = row >= col
    key_high, key_low = split(key_to)
    erase_high, erase_low = split(erase_to)
    for h, mask in enumerate((first, second)):
        head = 2 * pair + h
        a, b = key_high * mask, key_low * mask
        out = mm_t(left, rows(cols(a, a), cols(b, b)))
        out = out[:, :L] + out[:, L:]
        high, low = split(
            rows(jnp.where(strict, out[:L], 0.0), jnp.where(within, out[L:], 0.0))
        )
        s["on_values"][pair, :, h * L : h * L + L] = high
        s["on_values"][pair, :, (2 + h) * L : (3 + h) * L] = low
        a, b = erase_high * mask, erase_low * mask
        out = mm_t(left, rows(cols(a, a), cols(b, b)))
        out = out[:, :L] + out[:, L:]
        high, low = split(jnp.where(within, out[L:], 0.0))
        s["read_erase"][pair, :, h * L : h * L + L] = high
        s["read_erase"][pair, :, (2 + h) * L : (3 + h) * L] = low
        pairs = jnp.where(strict, out[:L], 0.0)
        high, low = split(pairs)
        s["lower"][head, :, :L] = high
        s["lower"][head, :, L:] = low
        next_to = (row // 2 == col // 2) & (row != col)
        s["inverse"][head] = (row == col).astype(F32) - jnp.where(next_to, pairs, 0.0)


def times(left, right):
    a, b = split(right)
    row = cols(a, b)
    out = mm(left, rows(row, row))
    return out[:, :L] + out[:, L:]


def refine(head0, count, level, s):
    row, col = grid_index()
    mask = ((row >> (level + 1)) == (col >> (level + 1))) & ((row >> level) != (col >> level))
    mask = mask.astype(BF16)
    mask = cols(mask, mask)
    held = [s["inverse"][head0 + i] for i in range(count)]
    below = [times(s["lower"][head0 + i] * mask, held[i]) for i in range(count)]
    for i in range(count):
        s["inverse"][head0 + i] = held[i] - times(cols(*split(held[i])), below[i])


def finish(pair, refs, s, out):
    lanes = pl.ds(pl.multiple_of(pair * L, L), L)
    first, second = half_masks(BF16)
    first2, second2 = half_masks(BF16, 2 * L)
    value = refs["value"][:, lanes]
    both = rows(value * first, value * second)
    seen = mm(s["on_values"][pair], rows(both, both))
    carried, local = seen[:L], seen[L:]

    def on_pair(left, right):
        high, low = split(right)
        high = rows(high * first2, high * second2)
        low = rows(low * first2, low * second2)
        return mm(left, rows(high, high)) + mm(left[:, : 2 * L], low)

    d0, d1 = split(s["inverse"][2 * pair]), split(s["inverse"][2 * pair + 1])
    solved = on_pair(
        cols(d0[0], d1[0], d0[1], d1[1]), cols(s["erase_start"][:, lanes], carried)
    )
    on_erase = on_pair(s["read_erase"][pair], solved)
    out["read_state"][:, lanes] = s["read_start"][:, lanes] - on_erase[:, :L]
    out["local"][:, lanes] = local - on_erase[:, L:]
    weights, taken = solved[:, :L], solved[:, L:]
    kh, kl = split(s["key_end"][:, lanes])
    eh, el = split(s["erase_end"][:, lanes])
    wh, wl = split(weights)
    th, tl = split(-taken)
    added = t_mm(rows(value, value, th, tl, th), rows(kh, kl, eh, eh, el))
    moved = t_mm(rows(wh, wl, wh), rows(eh, eh, el))
    decay = jnp.broadcast_to(s["decay"][:, lanes], (16, L))
    dh = decay.astype(BF16).astype(F32)
    dl = decay - dh
    low_half = lax.broadcasted_iota(jnp.int32, (HEAD, L), 1) < HEAD
    turn = lambda x: pltpu.roll(x, HEAD, 1)
    out["message"][2 * pair, :HEAD] = jnp.where(
        low_half, added[:HEAD], turn(moved[:HEAD])
    ).astype(BF16)
    out["message"][2 * pair, HEAD:] = jnp.where(low_half[:16], dh, turn(dl)).astype(BF16)
    out["message"][2 * pair + 1, :HEAD] = jnp.where(
        low_half, turn(added[HEAD:]), moved[HEAD:]
    ).astype(BF16)
    out["message"][2 * pair + 1, HEAD:] = jnp.where(low_half[:16], turn(dh), dl).astype(BF16)


def local_scratch(width):
    pairs = width // L
    wide = lambda: pltpu.VMEM((L, width), F32)
    return dict(
        squashed=pltpu.VMEM((L, L), BF16),
        read_start=wide(),
        erase_start=wide(),
        key_end=wide(),
        erase_end=wide(),
        decay=pltpu.VMEM((1, width), F32),
        on_values=pltpu.VMEM((pairs, 2 * L, 4 * L), BF16),
        read_erase=pltpu.VMEM((pairs, L, 4 * L), BF16),
        lower=pltpu.VMEM((2 * pairs, L, 2 * L), BF16),
        inverse=pltpu.VMEM((2 * pairs, L, L), F32),
    )


def read_pair(pair, read_state, local, states, gain, mix):
    lanes = pl.ds(pl.multiple_of(pair * L, L), L)
    low_half = lax.broadcasted_iota(jnp.int32, (HEAD // 2, L), 1) < HEAD
    turn = lambda x: pltpu.roll(x, HEAD, 1)
    a = states[2 * pair].astype(F32)
    b = states[2 * pair + 1].astype(F32)
    state = rows(
        jnp.where(low_half, a, 0.0),
        jnp.where(low_half, turn(a), 0.0),
        jnp.where(low_half, 0.0, turn(b)),
        jnp.where(low_half, 0.0, b),
    ).astype(BF16)
    readout = mm_t(cols(*split(read_state[:, lanes])), cols(state, state)) + local[:, lanes]
    row, col = grid_index()
    block = (row // HEAD == col // HEAD).astype(BF16)
    block = rows(block, block)
    centred = readout - mm(cols(*split(readout)), block) * (1.0 / HEAD)
    variance = mm(cols(*split(centred * centred)), block) * (1.0 / HEAD)
    mix[:, lanes] = (centred * lax.rsqrt(variance + 1.0) * gain[:, lanes]).astype(BF16)


def scratch(width, n_sp, n_dp):
    made = local_scratch(width)
    heads = width // HEAD
    steps = n_dp // 4
    dma = pltpu.SemaphoreType.DMA
    made.update(
        read_state=pltpu.VMEM((L, width), F32),
        local=pltpu.VMEM((L, width), F32),
        message=pltpu.VMEM((heads, MSG, L), BF16),
        got=pltpu.VMEM((n_sp, MSG, L), BF16),
        added=pltpu.VMEM((n_sp, HEAD, L), F32),
        moved=pltpu.VMEM((n_sp, HEAD, L), BF16),
        kept=pltpu.VMEM((n_sp, 8, L), F32),
        states=pltpu.VMEM((n_sp, HEAD // 2, L), BF16),
        starts=pltpu.VMEM((heads, HEAD // 2, L), BF16),
        mix=pltpu.VMEM((L, width), BF16),
        weights=pltpu.VMEM((n_dp, width, L), BF16),
        message_send=dma((n_sp,)),
        message_recv=dma((n_sp,)),
        state_send=dma((n_sp,)),
        state_recv=dma((n_sp,)),
        ring_send=dma((2 * steps,)),
        ring_recv=dma((2 * steps,)),
        twin_send=dma((2 * steps + 1,)),
        twin_recv=dma((2 * steps + 1,)),
    )
    return made


INPUTS = (
    "query",
    "key",
    "value",
    "decay_low",
    "rate_low",
    "decay_up",
    "rate_up",
    "base",
    "gain",
    "weight",
)
MESH = pl.DeviceIdType.MESH


def remote(src, dst, send, recv, **where):
    return pltpu.make_async_remote_copy(
        src_ref=src, dst_ref=dst, send_sem=send, recv_sem=recv, device_id=where, device_id_type=MESH
    )


def whole_kernel(*args, n_sp, n_dp, width, group=(2, 8, 2)):
    refs = dict(zip(INPUTS, args))
    out = args[len(INPUTS)]
    s = dict(zip(scratch(width, n_sp, n_dp), args[len(INPUTS) + 1 :]))
    pairs = width // L
    me = lax.axis_index("sp")
    me_dp = lax.axis_index("dp")
    core, y, ring = me_dp % 2, me_dp // 2, n_dp // 2
    steps = ring // 2
    twin = y * 2 + 1 - core
    at = lambda offset: ((y + offset + ring) % ring) * 2 + core

    barrier = pltpu.get_barrier_semaphore()

    @pl.loop(1, n_sp)
    def _(j):
        pl.semaphore_signal(
            barrier, inc=1, device_id={"sp": (me + j) % n_sp}, device_id_type=MESH
        )

    for peer in (twin, at(1), at(-1)):
        pl.semaphore_signal(barrier, inc=1, device_id={"dp": peer}, device_id_type=MESH)
    pl.semaphore_wait(barrier, n_sp + 2)

    def part(ref, way, step):
        if step < steps - 1:
            return ref
        half = width // 2
        return ref.at[pl.ds(way * half, half)]

    def ring_copy(way, step):
        block = at(-step if way == 0 else step)
        src = refs["weight"] if step == 0 else s["weights"].at[block]
        return remote(
            part(src, way, step),
            part(s["weights"].at[block], way, step),
            s["ring_send"].at[way * steps + step],
            s["ring_recv"].at[way * steps + step],
            dp=at(1 if way == 0 else -1),
        )

    def ring_arrival(way, step):
        block = at(-1 - step if way == 0 else 1 + step)
        here = part(s["weights"].at[block], way, step)
        return remote(
            here,
            here,
            s["ring_send"].at[way * steps + step],
            s["ring_recv"].at[way * steps + step],
            dp=at(1 if way == 0 else -1),
        )

    def twin_copy(way, step):
        index = way * steps + step
        here = part(s["weights"].at[at(-1 - step if way == 0 else 1 + step)], way, step)
        return remote(here, here, s["twin_send"].at[index], s["twin_recv"].at[index], dp=twin)

    def twin_arrival(way, step):
        index = way * steps + step
        offset = -1 - step if way == 0 else 1 + step
        block = ((y + offset + ring) % ring) * 2 + 1 - core
        here = part(s["weights"].at[block], way, step)
        return remote(here, here, s["twin_send"].at[index], s["twin_recv"].at[index], dp=twin)

    twin_own = remote(
        refs["weight"],
        s["weights"].at[me_dp],
        s["twin_send"].at[2 * steps],
        s["twin_recv"].at[2 * steps],
        dp=twin,
    )
    twin_first = remote(
        refs["weight"],
        s["weights"].at[twin],
        s["twin_send"].at[2 * steps],
        s["twin_recv"].at[2 * steps],
        dp=twin,
    )

    def forward(step):
        for way in range(2):
            ring_arrival(way, step).wait_recv()
            if step + 1 < steps:
                ring_copy(way, step + 1).start()
            twin_copy(way, step).start()

    for way in range(2):
        ring_copy(way, 0).start()
    twin_own.start()
    s["weights"][me_dp] = refs["weight"][...]

    s["squashed"][...] = jnp.tanh(refs["decay_low"][...].astype(F32)).astype(BF16)
    refs["squashed"] = s["squashed"]
    turned = lambda p: (p + me // 2) % pairs

    @pl.loop(0, pairs // group[0])
    def _(i):
        for j in range(group[0]):
            prepare(turned(i * group[0] + j), refs, s)

    forward(0)
    for level in range(1, 7):

        @pl.loop(0, 2 * pairs // group[1])
        def _(i):
            refine(i * group[1], group[1], level, s)

        if level == 3 and steps > 2:
            forward(1)

    def message_copy(head):
        return remote(
            s["message"].at[head],
            s["got"].at[me],
            s["message_send"].at[head],
            s["message_recv"].at[me],
            sp=head,
        )

    def send_messages(i):
        for j in range(group[2]):
            for h in range(2):
                head = 2 * turned(i * group[2] + j) + h

                @pl.when(head != me)
                def _():
                    message_copy(head).start()

    @pl.loop(0, pairs // group[2])
    def _(i):
        for j in range(group[2]):
            finish(turned(i * group[2] + j), refs, s, s)

        @pl.when(i > 0)
        def _():
            send_messages(i - 1)

    s["got"][me] = s["message"][me]
    send_messages(pairs // group[2] - 1)
    if steps > 3:
        forward(2)

    low_half = lax.broadcasted_iota(jnp.int32, (HEAD, L), 1) < HEAD
    turn = lambda x: pltpu.roll(x, HEAD, 1)

    def unpack(n):
        both = s["got"][n, :HEAD].astype(F32)
        s["added"][n] = both
        s["moved"][n] = jnp.where(low_half, turn(both), 0.0).astype(BF16)
        parts = s["got"][n, HEAD:].astype(F32)
        s["kept"][n] = (parts + turn(parts))[:8]

    unpack(me)

    @pl.loop(1, n_sp)
    def _(j):
        n = (me + j) % n_sp
        remote(
            s["got"].at[n],
            s["got"].at[n],
            s["message_send"].at[n],
            s["message_recv"].at[n],
            sp=n,
        ).wait_recv()
        unpack(n)

    def state_copy(n):
        return remote(
            s["states"].at[n],
            s["starts"].at[me],
            s["state_send"].at[n],
            s["state_recv"].at[me],
            sp=n,
        )

    def step(n, state):
        high, low = split(state)
        s["states"][n] = jnp.where(
            low_half[: HEAD // 2], state[: HEAD // 2], turn(state[HEAD // 2 :])
        ).astype(BF16)
        moved = mm(rows(high, low)[:, :HEAD], s["moved"][n])

        @pl.when((n > 0) & (n - 1 != me))
        def _():
            state_copy(n - 1).start()

        return state * s["kept"][n][:1] - (moved[:HEAD] + moved[HEAD:]) + s["added"][n]

    lax.fori_loop(0, n_sp, step, jnp.zeros((HEAD, L), F32))
    s["starts"][me] = s["states"][me]

    @pl.when(me != n_sp - 1)
    def _():
        state_copy(n_sp - 1).start()

    forward(steps - 1)

    @pl.loop(1, n_sp)
    def _(j):
        n = (me + j) % n_sp
        remote(
            s["starts"].at[n],
            s["starts"].at[n],
            s["state_send"].at[n],
            s["state_recv"].at[n],
            sp=n,
        ).wait_recv()

    @pl.loop(0, pairs // group[2])
    def _(i):
        for j in range(group[2]):
            read_pair(
                i * group[2] + j, s["read_state"], s["local"], s["starts"], refs["gain"], s["mix"]
            )

    twin_first.wait_recv()
    for way in range(2):
        for k in range(steps):
            twin_arrival(way, k).wait_recv()

    @pl.loop(0, n_dp // 2)
    def _(i):
        both = cols(s["weights"][2 * i], s["weights"][2 * i + 1])
        out[:, pl.ds(pl.multiple_of(i * 2 * L, 2 * L), 2 * L)] = mm(s["mix"][...], both).astype(
            BF16
        )

    twin_own.wait_send()
    for way in range(2):
        for k in range(steps):
            ring_copy(way, k).wait_send()
            twin_copy(way, k).wait_send()

    @pl.loop(1, n_sp)
    def _(j):
        n = (me + j) % n_sp
        message_copy(n).wait_send()
        state_copy(n).wait_send()


def solution(mesh):
    n_sp, n_dp = mesh.shape["sp"], mesh.shape["dp"]

    def per_device(
        query_rows,
        key_rows,
        value_rows,
        decay_low,
        rate_low,
        decay_up,
        rate_up,
        decay_base,
        norm_gain,
        out_weight,
    ):
        width = query_rows.shape[2]
        vmem = pl.BlockSpec(memory_space=pltpu.VMEM)
        out = pl.pallas_call(
            functools.partial(whole_kernel, n_sp=n_sp, n_dp=n_dp, width=width),
            out_shape=jax.ShapeDtypeStruct((L, n_dp * L), BF16),
            in_specs=[vmem] * len(INPUTS),
            out_specs=vmem,
            scratch_shapes=list(scratch(width, n_sp, n_dp).values()),
            compiler_params=pltpu.CompilerParams(
                collective_id=0, has_side_effects=True, vmem_limit_bytes=60 * 2**20
            ),
            name="mixer",
        )(
            query_rows[0],
            key_rows[0],
            value_rows[0],
            decay_low[0],
            rate_low[0],
            decay_up,
            rate_up,
            decay_base[None],
            norm_gain[None],
            out_weight,
        )
        return out[None]

    rows_spec = P("dp", "sp", None)
    return jax.shard_map(
        per_device,
        mesh=mesh,
        in_specs=(rows_spec,) * 5 + (P(), P(), P(), P(), P(None, "dp")),
        out_specs=rows_spec,
        check_vma=False,
    )
```

```python
import functools
import math

import jax
import jax.numpy as jnp
from jax import lax
from jax.experimental import pallas as pl
from jax.experimental.pallas import tpu as pltpu
from jax.sharding import PartitionSpec as P

HEAD = 64
L = 128
F32 = jnp.float32
BF16 = jnp.bfloat16
TAIL = 8
MSG = HEAD + TAIL
QUARTERS = 4
SPAN = 4


def split(x):
    high = x.astype(BF16)
    return high, (x - high.astype(F32)).astype(BF16)


def mm(a, b):
    return jnp.dot(a, b, preferred_element_type=F32)


def mm_t(a, b):
    return lax.dot_general(a, b, (((1,), (1,)), ((), ())), preferred_element_type=F32)


def t_mm(a, b):
    return lax.dot_general(a, b, (((0,), (0,)), ((), ())), preferred_element_type=F32)


def cols(*parts):
    return jnp.concatenate(parts, axis=1)


def rows(*parts):
    return jnp.concatenate(parts, axis=0)


def grid_index(n=L):
    return (
        lax.broadcasted_iota(jnp.int32, (n, n), 0),
        lax.broadcasted_iota(jnp.int32, (n, n), 1),
    )


def half_masks(dtype, width=L):
    lane = lax.broadcasted_iota(jnp.int32, (1, width), 1) % L
    return (lane < HEAD).astype(dtype), (lane >= HEAD).astype(dtype)


def prepare_group(chosen, refs, s):
    row, col = grid_index()
    first, second = half_masks(BF16)
    tri = (row >= col).astype(BF16)
    tri = cols(tri, tri)
    block = (row // HEAD == col // HEAD).astype(BF16)
    block = rows(block, block)
    held = []
    for pair in chosen:
        lanes = pl.ds(pl.multiple_of(pair * L, L), L)
        decay_pre = (
            refs["base"][:, lanes] + mm(s["squashed"][...], refs["decay_up"][:, lanes])
        ).astype(BF16)
        rate_pre = mm(refs["rate_low"][...], refs["rate_up"][:, lanes]).astype(BF16)
        log_decay = -math.exp(-0.5) / (1.0 + jnp.exp(-decay_pre.astype(F32)))
        rate = 1.0 / (1.0 + jnp.exp(-rate_pre.astype(F32)))
        running = mm(tri, rows(*split(log_decay)))
        key = refs["key"][:, lanes].astype(F32)
        total = mm(cols(*split(key * key)), block)
        held.append((pair, lanes, log_decay, rate, running, key, total))
    lefts = []
    for pair, lanes, log_decay, rate, running, key, total in held:
        before = running - log_decay
        centre = running[L // 2 : L // 2 + 1]
        final = running[L - 1 : L]
        query = refs["query"][:, lanes].astype(F32)
        unit = key * lax.rsqrt(1.0 + total)
        shrunk = jnp.exp(centre - running)
        read_mid = query * jnp.exp(running - centre)
        erase_from = unit * jnp.exp(before - centre)
        key_to = key * shrunk
        erase_to = unit * rate * shrunk
        up = jnp.exp(centre)
        down = jnp.exp(final - centre)
        s["read_start"][:, lanes] = read_mid * up
        s["erase_start"][:, lanes] = erase_from * up
        s["key_end"][:, lanes] = key_to * down
        s["erase_end"][:, lanes] = erase_to * down
        s["decay"][:, lanes] = jnp.exp(final)
        left = cols(*split(rows(erase_from, read_mid)))
        high, low = split(rows(key_to, erase_to))
        lefts.append((pair, left, high, low))
    for pair, left, high, low in lefts:
        for h, mask in enumerate((first, second)):
            a, b = high * mask, low * mask
            out = mm_t(left, cols(a, a)) + mm_t(left, cols(b, b))
            strict, within = s["strict"][...], s["within"][...]
            high_on, low_on = split(out[:L, :L] * strict)
            s["key_pairs"][pair, :, h * L : h * L + L] = high_on
            s["key_pairs"][pair, :, (2 + h) * L : (3 + h) * L] = low_on
            high_on, low_on = split(out[L:, :L] * within)
            s["read_keys"][pair, :, h * L : h * L + L] = high_on
            s["read_keys"][pair, :, (2 + h) * L : (3 + h) * L] = low_on
            high_on, low_on = split(out[L:, L:] * within)
            s["read_erase"][pair, :, h * L : h * L + L] = high_on
            s["read_erase"][pair, :, (2 + h) * L : (3 + h) * L] = low_on
            pairs = out[:L, L:] * strict
            high_on, low_on = split(pairs)
            head = 2 * pair + h
            s["lower"][head, :, :L] = high_on
            s["lower"][head, :, L:] = low_on
            s["inverse"][head] = s["eye"][...] - pairs * s["next_to"][...]


def times(left, right):
    a, b = split(right)
    row = cols(a, b)
    out = mm(left, rows(row, row))
    return out[:, :L] + out[:, L:]


def refine_group(chosen, level, s):
    held = [s["inverse"][head] for head in chosen]
    below = [
        times(s["lower"][head] * s["levels"][level], held[i]) for i, head in enumerate(chosen)
    ]
    for i, head in enumerate(chosen):
        s["inverse"][head] = held[i] - times(cols(*split(held[i])), below[i])


def fill_masks(s):
    row, col = grid_index()
    s["strict"][...] = (row > col).astype(F32)
    s["within"][...] = (row >= col).astype(F32)
    s["eye"][...] = (row == col).astype(F32)
    s["next_to"][...] = ((row // 2 == col // 2) & (row != col)).astype(F32)
    for level in range(1, 7):
        mask = (row >> (level + 1)) == (col >> (level + 1))
        mask = (mask & ((row >> level) != (col >> level))).astype(BF16)
        s["levels"][level - 1] = cols(mask, mask)


def on_pair(left, high, low):
    first, second = half_masks(BF16, 2 * L)
    high = rows(high * first, high * second)
    low = rows(low * first, low * second)
    return mm(left, rows(high, high)) + mm(left[:, : 2 * L], low)


def doubled(value):
    first, second = half_masks(BF16)
    both = rows(value * first, value * second)
    return rows(both, both)


def solve_group(chosen, refs, s):
    lanes_of = [pl.ds(pl.multiple_of(pair * L, L), L) for pair in chosen]
    carried = [
        mm(s["key_pairs"][pair], doubled(refs["value"][:, lanes]))
        for pair, lanes in zip(chosen, lanes_of)
    ]
    solved = []
    for pair, lanes, carry in zip(chosen, lanes_of, carried):
        d0, d1 = split(s["inverse"][2 * pair]), split(s["inverse"][2 * pair + 1])
        high, low = split(cols(s["erase_start"][:, lanes], carry))
        solved.append(split(on_pair(cols(d0[0], d1[0], d0[1], d1[1]), high, low)))
    low_half = lax.broadcasted_iota(jnp.int32, (HEAD, L), 1) < HEAD
    turn = lambda x: pltpu.roll(x, HEAD, 1)
    for pair, lanes, (high, low) in zip(chosen, lanes_of, solved):
        s["solved"][pair, :, : 2 * L] = high
        s["solved"][pair, :, 2 * L :] = low
        ends = cols(*split(s["erase_end"][:, lanes]))
        moved = t_mm(rows(high, low), rows(ends, ends))
        moved = moved[:, :L] + moved[:, L:]
        added = t_mm(refs["value"][:, lanes], cols(*split(s["key_end"][:, lanes])))
        added = added[:, :L] + added[:, L:] - moved[L:]
        moved = moved[:L]
        decay = jnp.broadcast_to(s["decay"][:, lanes], (TAIL, L))
        dh = decay.astype(BF16).astype(F32)
        dl = decay - dh
        s["message"][2 * pair, :HEAD] = jnp.where(
            low_half, added[:HEAD], turn(moved[:HEAD])
        ).astype(BF16)
        s["message"][2 * pair, HEAD:] = jnp.where(low_half[:TAIL], dh, turn(dl)).astype(BF16)
        s["message"][2 * pair + 1, :HEAD] = jnp.where(
            low_half, turn(added[HEAD:]), moved[HEAD:]
        ).astype(BF16)
        s["message"][2 * pair + 1, HEAD:] = jnp.where(low_half[:TAIL], turn(dh), dl).astype(BF16)


def local_group(chosen, refs, s):
    for pair in chosen:
        lanes = pl.ds(pl.multiple_of(pair * L, L), L)
        both = s["solved"][pair]
        on_erase = on_pair(s["read_erase"][pair], both[:, : 2 * L], both[:, 2 * L :])
        local = mm(s["read_keys"][pair], doubled(refs["value"][:, lanes]))
        s["read_state"][:, lanes] = s["read_start"][:, lanes] - on_erase[:, :L]
        s["local"][:, lanes] = local - on_erase[:, L:]


def read_group(chosen, refs, s):
    low_half = lax.broadcasted_iota(jnp.int32, (HEAD // 2, L), 1) < HEAD
    turn = lambda x: pltpu.roll(x, HEAD, 1)
    row, col = grid_index()
    block = (row // HEAD == col // HEAD).astype(BF16)
    block = rows(block, block)
    lanes_of = [pl.ds(pl.multiple_of(pair * L, L), L) for pair in chosen]
    readouts = []
    for pair, lanes in zip(chosen, lanes_of):
        a = s["starts"][2 * pair].astype(F32)
        b = s["starts"][2 * pair + 1].astype(F32)
        state = rows(
            jnp.where(low_half, a, 0.0),
            jnp.where(low_half, turn(a), 0.0),
            jnp.where(low_half, 0.0, turn(b)),
            jnp.where(low_half, 0.0, b),
        ).astype(BF16)
        readouts.append(
            mm_t(cols(*split(s["read_state"][:, lanes])), cols(state, state)) + s["local"][:, lanes]
        )
    centres = [x - mm(cols(*split(x)), block) * (1.0 / HEAD) for x in readouts]
    spreads = [mm(cols(*split(x * x)), block) * (1.0 / HEAD) for x in centres]
    for lanes, centred, variance in zip(lanes_of, centres, spreads):
        s["mix"][:, lanes] = (centred * lax.rsqrt(variance + 1.0) * refs["gain"][:, lanes]).astype(
            BF16
        )


def local_scratch(width):
    pairs = width // L
    wide = lambda: pltpu.VMEM((L, width), F32)
    return dict(
        squashed=pltpu.VMEM((L, L), BF16),
        read_start=wide(),
        erase_start=wide(),
        key_end=wide(),
        erase_end=wide(),
        decay=pltpu.VMEM((1, width), F32),
        key_pairs=pltpu.VMEM((pairs, L, 4 * L), BF16),
        read_keys=pltpu.VMEM((pairs, L, 4 * L), BF16),
        solved=pltpu.VMEM((pairs, L, 4 * L), BF16),
        strict=pltpu.VMEM((L, L), F32),
        within=pltpu.VMEM((L, L), F32),
        eye=pltpu.VMEM((L, L), F32),
        next_to=pltpu.VMEM((L, L), F32),
        levels=pltpu.VMEM((6, L, 2 * L), BF16),
        read_erase=pltpu.VMEM((pairs, L, 4 * L), BF16),
        lower=pltpu.VMEM((2 * pairs, L, 2 * L), BF16),
        inverse=pltpu.VMEM((2 * pairs, L, L), F32),
    )


def scratch(width, n_sp, n_dp):
    made = local_scratch(width)
    heads = width // HEAD
    chunks = n_dp // 4 * QUARTERS
    dma = pltpu.SemaphoreType.DMA
    made.update(
        read_state=pltpu.VMEM((L, width), F32),
        local=pltpu.VMEM((L, width), F32),
        message=pltpu.VMEM((heads, MSG, L), BF16),
        got=pltpu.VMEM((n_sp, MSG, L), BF16),
        added=pltpu.VMEM((n_sp, HEAD, L), F32),
        moved=pltpu.VMEM((n_sp, HEAD, L), BF16),
        kept=pltpu.VMEM((n_sp, 8, L), F32),
        prefix=pltpu.VMEM((n_sp, 2 * HEAD, L), F32),
        entry=pltpu.VMEM((n_sp // SPAN, HEAD, L), F32),
        states=pltpu.VMEM((n_sp, HEAD // 2, L), BF16),
        starts=pltpu.VMEM((heads, HEAD // 2, L), BF16),
        mix=pltpu.VMEM((L, width), BF16),
        weights=pltpu.VMEM((n_dp, width, L), BF16),
        message_send=dma((n_sp,)),
        message_recv=dma((n_sp,)),
        state_send=dma((n_sp,)),
        state_recv=dma((n_sp,)),
        ring_send=dma((2 * chunks,)),
        ring_recv=dma((2 * chunks,)),
        twin_send=dma((2 * chunks + 1,)),
        twin_recv=dma((2 * chunks + 1,)),
    )
    return made


INPUTS = (
    "query",
    "key",
    "value",
    "decay_low",
    "rate_low",
    "decay_up",
    "rate_up",
    "base",
    "gain",
    "weight",
)
MESH = pl.DeviceIdType.MESH


def remote(src, dst, send, recv, **where):
    return pltpu.make_async_remote_copy(
        src_ref=src, dst_ref=dst, send_sem=send, recv_sem=recv, device_id=where, device_id_type=MESH
    )


def whole_kernel(*args, n_sp, n_dp, width, schedule):
    refs = dict(zip(INPUTS, args))
    out = args[len(INPUTS)]
    s = dict(zip(scratch(width, n_sp, n_dp), args[len(INPUTS) + 1 :]))
    pairs = width // L
    half = pairs // 2
    me = lax.axis_index("sp")
    me_dp = lax.axis_index("dp")
    core, y, ring = me_dp % 2, me_dp // 2, n_dp // 2
    steps = ring // 2
    twin = y * 2 + 1 - core
    at = lambda offset, c: ((y + offset + ring) % ring) * 2 + c
    barrier = pltpu.get_barrier_semaphore()

    def greet():
        @pl.loop(1, n_sp)
        def _(j):
            pl.semaphore_signal(
                barrier, inc=1, device_id={"sp": (me + j) % n_sp}, device_id_type=MESH
            )

        for peer in (twin, at(1, core), at(-1, core)):
            pl.semaphore_signal(barrier, inc=1, device_id={"dp": peer}, device_id_type=MESH)

    def met():
        pl.semaphore_wait(barrier, n_sp + 2)

    order = [
        [
            (step, quarter)
            for step in range(steps)
            for quarter in ((0, 1, 2, 3), (2, 3, 0, 1))[way][: 4 if step < steps - 1 else 2]
        ]
        for way in range(2)
    ]
    chunk = width // QUARTERS
    moved = {"chunks": 0}

    def piece(ref, quarter):
        return ref.at[pl.ds(quarter * chunk, chunk)]

    def ring_copy(way, step, quarter):
        block = s["weights"].at[at(-step if way == 0 else step, core)]
        src = refs["weight"] if step == 0 else block
        index = (way * steps + step) * QUARTERS + quarter
        return remote(
            piece(src, quarter),
            piece(block, quarter),
            s["ring_send"].at[index],
            s["ring_recv"].at[index],
            dp=at(1 if way == 0 else -1, core),
        )

    def arrival(way, step, quarter, kind):
        offset = -1 - step if way == 0 else 1 + step
        here = s["weights"].at[at(offset, core if kind == "ring" else 1 - core)]
        here = piece(here, quarter)
        index = (way * steps + step) * QUARTERS + quarter
        peer = twin if kind == "twin" else at(1 if way == 0 else -1, core)
        return remote(
            here, here, s[kind + "_send"].at[index], s[kind + "_recv"].at[index], dp=peer
        )

    def twin_copy(way, step, quarter):
        offset = -1 - step if way == 0 else 1 + step
        here = piece(s["weights"].at[at(offset, core)], quarter)
        index = (way * steps + step) * QUARTERS + quarter
        return remote(here, here, s["twin_send"].at[index], s["twin_recv"].at[index], dp=twin)

    def twin_own(block):
        return remote(
            refs["weight"],
            s["weights"].at[block],
            s["twin_send"].at[2 * steps * QUARTERS],
            s["twin_recv"].at[2 * steps * QUARTERS],
            dp=twin,
        )

    def advance(count):
        count = min(count, len(order[0]))
        for place in range(moved["chunks"], count):
            for way in range(2):
                step, quarter = order[way][place]
                arrival(way, step, quarter, "ring").wait_recv()
                if (step + 1, quarter) in order[way]:
                    ring_copy(way, step + 1, quarter).start()
                twin_copy(way, step, quarter).start()
        moved["chunks"] = max(count, moved["chunks"])

    def start_weights():
        for place in range(QUARTERS if steps > 1 else 2):
            for way in range(2):
                ring_copy(way, *order[way][place]).start()
        twin_own(me_dp).start()
        s["weights"][me_dp] = refs["weight"][...]

    def wait_weights():
        advance(len(order[0]))
        twin_own(twin).wait_recv()
        for way in range(2):
            for place in order[way]:
                arrival(way, *place, "twin").wait_recv()

    def pair_at(i):
        offset = half + jnp.where(i % 2 == 1, -((i + 1) // 2), i // 2)
        return (me // 2 + offset) % pairs

    def squash():
        s["squashed"][...] = jnp.tanh(refs["decay_low"][...].astype(F32)).astype(BF16)
        fill_masks(s)

    def in_groups(first, count, size, body):
        size = math.gcd(count, size)

        @pl.loop(0, count // size)
        def _(i):
            body([pair_at(first + i * size + j) for j in range(size)])

    def prepare_half(first):
        in_groups(first, half, 4, lambda chosen: prepare_group(chosen, refs, s))

    def refine_half(first):
        chosen = [pair_at(jnp.int32(first + j)) for j in range(half)]
        heads = [2 * pair + h for pair in chosen for h in range(2)]

        @pl.loop(0, 6)
        def _(level):
            refine_group(heads, level, s)

    def message_copy(head):
        return remote(
            s["message"].at[head],
            s["got"].at[me],
            s["message_send"].at[head],
            s["message_recv"].at[me],
            sp=head,
        )

    def send_messages(chosen):
        for pair in chosen:
            for h in range(2):
                head = 2 * pair + h

                @pl.when(head != me)
                def _():
                    message_copy(head).start()

    def solve_half(first):
        size = math.gcd(half, 4)

        @pl.loop(0, half // size)
        def _(i):
            chosen = [pair_at(first + i * size + j) for j in range(size)]
            solve_group(chosen, refs, s)
            send_messages(chosen)

    low_half = lax.broadcasted_iota(jnp.int32, (HEAD, L), 1) < HEAD
    turn = lambda x: pltpu.roll(x, HEAD, 1)

    def unpack(n):
        both = s["got"][n, :HEAD].astype(F32)
        s["added"][n] = both
        s["moved"][n] = jnp.where(low_half, turn(both), 0.0).astype(BF16)
        parts = s["got"][n, HEAD:].astype(F32)
        s["kept"][n] = parts + turn(parts)

    def peer_at(j):
        offset = n_sp // 2 + jnp.where(j % 2 == 1, -((j + 1) // 2), j // 2)
        return (me + offset) % n_sp

    def unpack_all():
        s["got"][me] = s["message"][me]
        unpack(me)

        @pl.loop(0, n_sp - 1)
        def _(j):
            n = peer_at(j)
            remote(
                s["got"].at[n],
                s["got"].at[n],
                s["message_send"].at[n],
                s["message_recv"].at[n],
                sp=n,
            ).wait_recv()
            unpack(n)

    def state_copy(n):
        return remote(
            s["states"].at[n],
            s["starts"].at[me],
            s["state_send"].at[n],
            s["state_recv"].at[me],
            sp=n,
        )

    def on_state(state, x):
        high, low = split(x[HEAD:, :HEAD])
        left = rows(*split(state[:, :HEAD]))
        a = mm(left, high)
        return a[:HEAD] + a[HEAD:] + mm(left[:HEAD], low)

    def scan_all():
        spans = n_sp // SPAN
        row = lax.broadcasted_iota(jnp.int32, (2 * HEAD, L), 0)
        col = lax.broadcasted_iota(jnp.int32, (2 * HEAD, L), 1)
        start = (row == col + HEAD).astype(F32)
        xs = [start] * spans
        for j in range(SPAN):
            outs = []
            for g in range(spans):
                n = g * SPAN + j
                s["prefix"][n] = xs[g]
                outs.append(mm(rows(*split(xs[g][:, :HEAD])), s["moved"][n]))
            for g in range(spans):
                n = g * SPAN + j
                a = outs[g][: 2 * HEAD] + outs[g][2 * HEAD :]
                x = xs[g] * s["kept"][n][:1] - a
                xs[g] = rows(x[:HEAD] + s["added"][n], x[HEAD:])
        state = jnp.zeros((HEAD, HEAD), F32)
        for g in range(spans):
            s["entry"][g, :, :HEAD] = state
            if g + 1 < spans:
                state = on_state(state, xs[g]) + xs[g][:HEAD, :HEAD]

    def emit(n):
        x = s["prefix"][n]
        state = on_state(s["entry"][n // SPAN], x) + x[:HEAD, :HEAD]
        state = cols(state, state)
        s["states"][n] = jnp.where(
            low_half[: HEAD // 2], state[: HEAD // 2], state[HEAD // 2 :]
        ).astype(BF16)

    def emit_all():
        size = 4

        @pl.loop(0, n_sp // size)
        def _(i):
            for j in range(size):
                emit(peer_at(i * size + j))
            for j in range(size):
                n = peer_at(i * size + j)

                @pl.when(n != me)
                def _():
                    state_copy(n).start()

        s["starts"][me] = s["states"][me]

    def local_all():
        in_groups(0, pairs, 4, lambda chosen: local_group(chosen, refs, s))

    def wait_starts():
        @pl.loop(0, n_sp - 1)
        def _(j):
            n = peer_at(j)
            remote(
                s["starts"].at[n],
                s["starts"].at[n],
                s["state_send"].at[n],
                s["state_recv"].at[n],
                sp=n,
            ).wait_recv()

    def read_all():
        in_groups(0, pairs, 4, lambda chosen: read_group(chosen, refs, s))

    def project():
        @pl.loop(0, n_dp // 2)
        def _(i):
            both = cols(s["weights"][2 * i], s["weights"][2 * i + 1])
            out[:, pl.ds(pl.multiple_of(i * 2 * L, 2 * L), 2 * L)] = mm(
                s["mix"][...], both
            ).astype(BF16)

    def drain():
        twin_own(me_dp).wait_send()
        for way in range(2):
            for place in order[way]:
                ring_copy(way, *place).wait_send()
                twin_copy(way, *place).wait_send()

        @pl.loop(1, n_sp)
        def _(j):
            n = (me + j) % n_sp
            message_copy(n).wait_send()
            state_copy(n).wait_send()

    phases = [
        ("greet", greet),
        ("squash", squash),
        ("met", met),
        ("weights", start_weights),
        ("prepare0", functools.partial(prepare_half, 0)),
        ("refine0", functools.partial(refine_half, 0)),
        ("solve0", functools.partial(solve_half, 0)),
        ("prepare1", functools.partial(prepare_half, half)),
        ("refine1", functools.partial(refine_half, half)),
        ("solve1", functools.partial(solve_half, half)),
        ("unpack", unpack_all),
        ("scan", scan_all),
        ("emit", emit_all),
        ("local", local_all),
        ("starts", wait_starts),
        ("read", read_all),
        ("whole", wait_weights),
        ("project", project),
        ("drain", drain),
    ]
    for name, phase in phases:
        with jax.named_scope(name):
            phase()
        if name in schedule:
            with jax.named_scope("pass_" + name):
                advance(schedule[name])


SCHEDULE = {
    "prepare0": 1,
    "refine0": 2,
    "solve0": 3,
    "prepare1": 4,
    "refine1": 6,
    "solve1": 7,
    "unpack": 8,
    "emit": 9,
    "local": 10,
    "starts": 12,
}


def solution(mesh):
    n_sp, n_dp = mesh.shape["sp"], mesh.shape["dp"]

    def per_device(
        query_rows,
        key_rows,
        value_rows,
        decay_low,
        rate_low,
        decay_up,
        rate_up,
        decay_base,
        norm_gain,
        out_weight,
    ):
        width = query_rows.shape[2]
        vmem = pl.BlockSpec(memory_space=pltpu.VMEM)
        out = pl.pallas_call(
            functools.partial(
                whole_kernel, n_sp=n_sp, n_dp=n_dp, width=width, schedule=SCHEDULE
            ),
            out_shape=jax.ShapeDtypeStruct((L, n_dp * L), BF16),
            in_specs=[vmem] * len(INPUTS),
            out_specs=vmem,
            scratch_shapes=list(scratch(width, n_sp, n_dp).values()),
            compiler_params=pltpu.CompilerParams(
                collective_id=0, has_side_effects=True, vmem_limit_bytes=60 * 2**20
            ),
            name="mixer",
        )(
            query_rows[0],
            key_rows[0],
            value_rows[0],
            decay_low[0],
            rate_low[0],
            decay_up,
            rate_up,
            decay_base[None],
            norm_gain[None],
            out_weight,
        )
        return out[None]

    rows_spec = P("dp", "sp", None)
    return jax.shard_map(
        per_device,
        mesh=mesh,
        in_specs=(rows_spec,) * 5 + (P(), P(), P(), P(), P(None, "dp")),
        out_specs=rows_spec,
        check_vma=False,
    )
```

```python
import functools
import math

import jax
import jax.numpy as jnp
from jax import lax
from jax.experimental import pallas as pl
from jax.experimental.pallas import tpu as pltpu
from jax.sharding import PartitionSpec as P

HEAD = 64
L = 128
F32 = jnp.float32
BF16 = jnp.bfloat16
TAIL = 8
MSG = HEAD + TAIL
QUARTERS = 4
SPAN = 4
SHARED = 3
ALONG_X = 4


def split(x):
    high = x.astype(BF16)
    return high, (x - high.astype(F32)).astype(BF16)


def mm(a, b):
    return jnp.dot(a, b, preferred_element_type=F32)


def mm_t(a, b):
    return lax.dot_general(a, b, (((1,), (1,)), ((), ())), preferred_element_type=F32)


def t_mm(a, b):
    return lax.dot_general(a, b, (((0,), (0,)), ((), ())), preferred_element_type=F32)


def cols(*parts):
    return jnp.concatenate(parts, axis=1)


def rows(*parts):
    return jnp.concatenate(parts, axis=0)


def grid_index(n=L):
    return (
        lax.broadcasted_iota(jnp.int32, (n, n), 0),
        lax.broadcasted_iota(jnp.int32, (n, n), 1),
    )


def half_masks(dtype, width=L):
    lane = lax.broadcasted_iota(jnp.int32, (1, width), 1) % L
    return (lane < HEAD).astype(dtype), (lane >= HEAD).astype(dtype)


def prepare_group(chosen, refs, s):
    row, col = grid_index()
    first, second = half_masks(BF16)
    tri = (row >= col).astype(BF16)
    tri = cols(tri, tri)
    block = (row // HEAD == col // HEAD).astype(BF16)
    block = rows(block, block)
    held = []
    for pair in chosen:
        lanes = pl.ds(pl.multiple_of(pair * L, L), L)
        decay_pre = (
            refs["base"][:, lanes] + mm(s["squashed"][...], refs["decay_up"][:, lanes])
        ).astype(BF16)
        rate_pre = mm(refs["rate_low"][...], refs["rate_up"][:, lanes]).astype(BF16)
        log_decay = -math.exp(-0.5) / (1.0 + jnp.exp(-decay_pre.astype(F32)))
        rate = 1.0 / (1.0 + jnp.exp(-rate_pre.astype(F32)))
        running = mm(tri, rows(*split(log_decay)))
        key = refs["key"][:, lanes].astype(F32)
        total = mm(cols(*split(key * key)), block)
        held.append((pair, lanes, log_decay, rate, running, key, total))
    lefts = []
    for pair, lanes, log_decay, rate, running, key, total in held:
        before = running - log_decay
        centre = running[L // 2 : L // 2 + 1]
        final = running[L - 1 : L]
        query = refs["query"][:, lanes].astype(F32)
        unit = key * lax.rsqrt(1.0 + total)
        shrunk = jnp.exp(centre - running)
        read_mid = query * jnp.exp(running - centre)
        erase_from = unit * jnp.exp(before - centre)
        key_to = key * shrunk
        erase_to = unit * rate * shrunk
        up = jnp.exp(centre)
        down = jnp.exp(final - centre)
        s["read_start"][:, lanes] = read_mid * up
        s["erase_start"][:, lanes] = erase_from * up
        s["key_end"][:, lanes] = key_to * down
        s["erase_end"][:, lanes] = erase_to * down
        s["decay"][:, lanes] = jnp.exp(final)
        left = cols(*split(rows(erase_from, read_mid)))
        high, low = split(rows(key_to, erase_to))
        lefts.append((pair, left, high, low))
    for pair, left, high, low in lefts:
        for h, mask in enumerate((first, second)):
            a, b = high * mask, low * mask
            out = mm_t(left, cols(a, a)) + mm_t(left, cols(b, b))
            strict, within = s["strict"][...], s["within"][...]
            high_on, low_on = split(out[:L, :L] * strict)
            s["key_pairs"][pair, :, h * L : h * L + L] = high_on
            s["key_pairs"][pair, :, (2 + h) * L : (3 + h) * L] = low_on
            high_on, low_on = split(out[L:, :L] * within)
            s["read_keys"][pair, :, h * L : h * L + L] = high_on
            s["read_keys"][pair, :, (2 + h) * L : (3 + h) * L] = low_on
            high_on, low_on = split(out[L:, L:] * within)
            s["read_erase"][pair, :, h * L : h * L + L] = high_on
            s["read_erase"][pair, :, (2 + h) * L : (3 + h) * L] = low_on
            pairs = out[:L, L:] * strict
            high_on, low_on = split(pairs)
            head = 2 * pair + h
            s["lower"][head, :, :L] = high_on
            s["lower"][head, :, L:] = low_on
            s["inverse"][head] = s["eye"][...] - pairs * s["next_to"][...]


def times(left, right):
    a, b = split(right)
    row = cols(a, b)
    out = mm(left, rows(row, row))
    return out[:, :L] + out[:, L:]


def refine_group(chosen, level, s):
    held = [s["inverse"][head] for head in chosen]
    below = [
        times(s["lower"][head] * s["levels"][level], held[i]) for i, head in enumerate(chosen)
    ]
    for i, head in enumerate(chosen):
        s["inverse"][head] = held[i] - times(cols(*split(held[i])), below[i])


def fill_masks(s):
    row, col = grid_index()
    s["strict"][...] = (row > col).astype(F32)
    s["within"][...] = (row >= col).astype(F32)
    s["eye"][...] = (row == col).astype(F32)
    s["next_to"][...] = ((row // 2 == col // 2) & (row != col)).astype(F32)
    for level in range(1, 7):
        mask = (row >> (level + 1)) == (col >> (level + 1))
        mask = (mask & ((row >> level) != (col >> level))).astype(BF16)
        s["levels"][level - 1] = cols(mask, mask)


def on_pair(left, high, low):
    first, second = half_masks(BF16, 2 * L)
    high = rows(high * first, high * second)
    low = rows(low * first, low * second)
    return mm(left, rows(high, high)) + mm(left[:, : 2 * L], low)


def doubled(value):
    first, second = half_masks(BF16)
    both = rows(value * first, value * second)
    return rows(both, both)


def solve_group(chosen, refs, s):
    lanes_of = [pl.ds(pl.multiple_of(pair * L, L), L) for pair in chosen]
    carried = [
        mm(s["key_pairs"][pair], doubled(refs["value"][:, lanes]))
        for pair, lanes in zip(chosen, lanes_of)
    ]
    solved = []
    for pair, lanes, carry in zip(chosen, lanes_of, carried):
        d0, d1 = split(s["inverse"][2 * pair]), split(s["inverse"][2 * pair + 1])
        high, low = split(cols(s["erase_start"][:, lanes], carry))
        solved.append(split(on_pair(cols(d0[0], d1[0], d0[1], d1[1]), high, low)))
    low_half = lax.broadcasted_iota(jnp.int32, (HEAD, L), 1) < HEAD
    turn = lambda x: pltpu.roll(x, HEAD, 1)
    for pair, lanes, (high, low) in zip(chosen, lanes_of, solved):
        s["solved"][pair, :, : 2 * L] = high
        s["solved"][pair, :, 2 * L :] = low
        ends = cols(*split(s["erase_end"][:, lanes]))
        moved = t_mm(rows(high, low), rows(ends, ends))
        moved = moved[:, :L] + moved[:, L:]
        added = t_mm(refs["value"][:, lanes], cols(*split(s["key_end"][:, lanes])))
        added = added[:, :L] + added[:, L:] - moved[L:]
        moved = moved[:L]
        decay = jnp.broadcast_to(s["decay"][:, lanes], (TAIL, L))
        dh = decay.astype(BF16).astype(F32)
        dl = decay - dh
        s["message"][2 * pair, :HEAD] = jnp.where(
            low_half, added[:HEAD], turn(moved[:HEAD])
        ).astype(BF16)
        s["message"][2 * pair, HEAD:] = jnp.where(low_half[:TAIL], dh, turn(dl)).astype(BF16)
        s["message"][2 * pair + 1, :HEAD] = jnp.where(
            low_half, turn(added[HEAD:]), moved[HEAD:]
        ).astype(BF16)
        s["message"][2 * pair + 1, HEAD:] = jnp.where(low_half[:TAIL], turn(dh), dl).astype(BF16)


def local_group(chosen, refs, s):
    for pair in chosen:
        lanes = pl.ds(pl.multiple_of(pair * L, L), L)
        both = s["solved"][pair]
        on_erase = on_pair(s["read_erase"][pair], both[:, : 2 * L], both[:, 2 * L :])
        local = mm(s["read_keys"][pair], doubled(refs["value"][:, lanes]))
        s["read_state"][:, lanes] = s["read_start"][:, lanes] - on_erase[:, :L]
        s["local"][:, lanes] = local - on_erase[:, L:]


def read_group(chosen, refs, s):
    low_half = lax.broadcasted_iota(jnp.int32, (HEAD // 2, L), 1) < HEAD
    turn = lambda x: pltpu.roll(x, HEAD, 1)
    row, col = grid_index()
    block = (row // HEAD == col // HEAD).astype(BF16)
    block = rows(block, block)
    lanes_of = [pl.ds(pl.multiple_of(pair * L, L), L) for pair in chosen]
    readouts = []
    for pair, lanes in zip(chosen, lanes_of):
        a = s["starts"][2 * pair].astype(F32)
        b = s["starts"][2 * pair + 1].astype(F32)
        state = rows(
            jnp.where(low_half, a, 0.0),
            jnp.where(low_half, turn(a), 0.0),
            jnp.where(low_half, 0.0, turn(b)),
            jnp.where(low_half, 0.0, b),
        ).astype(BF16)
        readouts.append(
            mm_t(cols(*split(s["read_state"][:, lanes])), cols(state, state)) + s["local"][:, lanes]
        )
    centres = [x - mm(cols(*split(x)), block) * (1.0 / HEAD) for x in readouts]
    spreads = [mm(cols(*split(x * x)), block) * (1.0 / HEAD) for x in centres]
    for lanes, centred, variance in zip(lanes_of, centres, spreads):
        s["mix"][:, lanes] = (centred * lax.rsqrt(variance + 1.0) * refs["gain"][:, lanes]).astype(
            BF16
        )


def local_scratch(width):
    pairs = width // L
    wide = lambda: pltpu.VMEM((L, width), F32)
    return dict(
        squashed=pltpu.VMEM((L, L), BF16),
        read_start=wide(),
        erase_start=wide(),
        key_end=wide(),
        erase_end=wide(),
        decay=pltpu.VMEM((1, width), F32),
        key_pairs=pltpu.VMEM((pairs, L, 4 * L), BF16),
        read_keys=pltpu.VMEM((pairs, L, 4 * L), BF16),
        solved=pltpu.VMEM((pairs, L, 4 * L), BF16),
        strict=pltpu.VMEM((L, L), F32),
        within=pltpu.VMEM((L, L), F32),
        eye=pltpu.VMEM((L, L), F32),
        next_to=pltpu.VMEM((L, L), F32),
        levels=pltpu.VMEM((6, L, 2 * L), BF16),
        read_erase=pltpu.VMEM((pairs, L, 4 * L), BF16),
        lower=pltpu.VMEM((2 * pairs, L, 2 * L), BF16),
        inverse=pltpu.VMEM((2 * pairs, L, L), F32),
    )


INPUTS = (
    "query",
    "key",
    "value",
    "decay_low",
    "rate_low",
    "decay_up",
    "rate_up",
    "base",
    "gain",
    "weight",
)


def scratch(width, n_sp, n_dp):
    made = local_scratch(width)
    heads = width // HEAD
    chunks = n_dp // 4 * QUARTERS
    dma = pltpu.SemaphoreType.DMA
    made.update(
        read_state=pltpu.VMEM((L, width), F32),
        local=pltpu.VMEM((L, width), F32),
        message=pltpu.VMEM((heads, MSG, L), BF16),
        got=pltpu.VMEM((n_sp, MSG, L), BF16),
        added=pltpu.VMEM((n_sp, HEAD, L), F32),
        moved=pltpu.VMEM((n_sp, HEAD, L), BF16),
        kept=pltpu.VMEM((n_sp, 8, L), F32),
        prefix=pltpu.VMEM((n_sp, 2 * HEAD, L), F32),
        entry=pltpu.VMEM((n_sp // SPAN, HEAD, L), F32),
        states=pltpu.VMEM((n_sp, HEAD // 2, L), BF16),
        starts=pltpu.VMEM((heads, HEAD // 2, L), BF16),
        mix=pltpu.VMEM((L, width), BF16),
        weights=pltpu.VMEM((n_dp, width, L), BF16),
        query=pltpu.VMEM((L, width), BF16),
        key=pltpu.VMEM((L, width), BF16),
        value=pltpu.VMEM((L, width), BF16),
        decay_low=pltpu.VMEM((L, L), BF16),
        rate_low=pltpu.VMEM((L, L), BF16),
        decay_up=pltpu.VMEM((L, width), BF16),
        rate_up=pltpu.VMEM((L, width), BF16),
        base=pltpu.VMEM((1, width), F32),
        gain=pltpu.VMEM((1, width), F32),
        fetched=dma((len(INPUTS),)),
        x_send=dma((2 * chunks,)),
        x_recv=dma((2 * chunks,)),
        message_send=dma((n_sp,)),
        message_recv=dma((n_sp,)),
        state_send=dma((n_sp,)),
        state_recv=dma((n_sp,)),
        ring_send=dma((2 * chunks,)),
        ring_recv=dma((2 * chunks,)),
        twin_send=dma((2 * chunks + 1,)),
        twin_recv=dma((2 * chunks + 1,)),
    )
    return made


MESH = pl.DeviceIdType.MESH


def remote(src, dst, send, recv, **where):
    return pltpu.make_async_remote_copy(
        src_ref=src, dst_ref=dst, send_sem=send, recv_sem=recv, device_id=where, device_id_type=MESH
    )


def whole_kernel(*args, n_sp, n_dp, width, schedule):
    given = dict(zip(INPUTS, args))
    out = args[len(INPUTS)]
    s = dict(zip(scratch(width, n_sp, n_dp), args[len(INPUTS) + 1 :]))
    refs = {name: s[name] for name in INPUTS if name != "weight"}
    pairs = width // L
    half = pairs // 2
    me = lax.axis_index("sp")
    me_dp = lax.axis_index("dp")
    core, y, ring = me_dp % 2, me_dp // 2, n_dp // 2
    steps = ring // 2
    twin = y * 2 + 1 - core
    at = lambda offset, c: ((y + offset + ring) % ring) * 2 + c
    along = math.gcd(n_sp, ALONG_X)
    x = me % along
    barrier = pltpu.get_barrier_semaphore()

    def fetch(name):
        target = s["weights"].at[me_dp] if name == "weight" else s[name]
        return pltpu.make_async_copy(given[name], target, s["fetched"].at[INPUTS.index(name)])

    def fetch_all():
        for name in ("decay_low", "decay_up", "base", "rate_low", "rate_up", "key", "query"):
            fetch(name).start()
        for name in ("value", "gain", "weight"):
            fetch(name).start()

    def greet():
        @pl.loop(1, n_sp)
        def _(j):
            pl.semaphore_signal(
                barrier, inc=1, device_id={"sp": (me + j) % n_sp}, device_id_type=MESH
            )

        for peer in (twin, at(1, core), at(-1, core)):
            pl.semaphore_signal(barrier, inc=1, device_id={"dp": peer}, device_id_type=MESH)

    def met():
        pl.semaphore_wait(barrier, n_sp + 2)

    order = [
        [
            (step, quarter)
            for step in range(steps)
            for quarter in (
                ((SHARED, 0, 1, 2), (SHARED, 2, 0, 1))[way]
                if step < steps - 1
                else ((0, 1), (SHARED, 2))[way]
            )
        ]
        for way in range(2)
    ]
    chunk = width // QUARTERS
    moved = {"chunks": 0}

    share = chunk // along

    def piece(ref, quarter):
        if quarter != SHARED:
            return ref.at[pl.ds(quarter * chunk, chunk)]
        return ref.at[pl.ds(pl.multiple_of(SHARED * chunk + x * share, share), share)]

    def whole_piece(ref, quarter):
        return ref.at[pl.ds(quarter * chunk, chunk)]

    def ring_copy(way, step, quarter):
        block = s["weights"].at[at(-step if way == 0 else step, core)]
        src = given["weight"] if step == 0 else block
        index = (way * steps + step) * QUARTERS + quarter
        return remote(
            piece(src, quarter),
            piece(block, quarter),
            s["ring_send"].at[index],
            s["ring_recv"].at[index],
            dp=at(1 if way == 0 else -1, core),
        )

    def arrival(way, step, quarter, kind):
        offset = -1 - step if way == 0 else 1 + step
        here = s["weights"].at[at(offset, core if kind == "ring" else 1 - core)]
        here = (piece if kind == "ring" else whole_piece)(here, quarter)
        index = (way * steps + step) * QUARTERS + quarter
        peer = twin if kind == "twin" else at(1 if way == 0 else -1, core)
        return remote(
            here, here, s[kind + "_send"].at[index], s[kind + "_recv"].at[index], dp=peer
        )

    def twin_copy(way, step, quarter):
        offset = -1 - step if way == 0 else 1 + step
        here = whole_piece(s["weights"].at[at(offset, core)], quarter)
        index = (way * steps + step) * QUARTERS + quarter
        return remote(here, here, s["twin_send"].at[index], s["twin_recv"].at[index], dp=twin)

    def twin_own(block):
        return remote(
            given["weight"],
            s["weights"].at[block],
            s["twin_send"].at[2 * steps * QUARTERS],
            s["twin_recv"].at[2 * steps * QUARTERS],
            dp=twin,
        )

    def x_copy(way, step, k, theirs=False):
        offset = -1 - step if way == 0 else 1 + step
        start = SHARED * chunk + ((x - k + along) % along if theirs else x) * share
        here = s["weights"].at[at(offset, core)]
        here = here.at[pl.ds(pl.multiple_of(start, share), share)]
        index = (way * steps + step) * QUARTERS + k
        return remote(
            here, here, s["x_send"].at[index], s["x_recv"].at[index], sp=me - x + (x + k) % along
        )

    def join(way, step):
        for k in range(1, along):
            x_copy(way, step, k, True).wait_recv()
        twin_copy(way, step, SHARED).start()

    def advance(count):
        count = min(count, len(order[0]))
        for place in range(moved["chunks"], count):
            for way in range(2):
                step, quarter = order[way][place]
                arrival(way, step, quarter, "ring").wait_recv()
                if (step + 1, quarter) in order[way]:
                    ring_copy(way, step + 1, quarter).start()
                if quarter == SHARED:
                    for k in range(1, along):
                        x_copy(way, step, k).start()
                    moved[(way, step)] = place + 2
                else:
                    twin_copy(way, step, quarter).start()
            for way in range(2):
                for step in range(steps):
                    if moved.get((way, step)) == place:
                        join(way, step)
                        moved[(way, step)] = -1
        moved["chunks"] = max(count, moved["chunks"])

    def start_weights():
        for place in range(QUARTERS if steps > 1 else 2):
            for way in range(2):
                ring_copy(way, *order[way][place]).start()
        twin_own(me_dp).start()

    def project_at(offset):
        both = cols(s["weights"][at(offset, 0)], s["weights"][at(offset, 1)])
        where = pl.ds(pl.multiple_of(at(offset, 0) * L, 2 * L), 2 * L)
        out[:, where] = mm(s["mix"][...], both).astype(BF16)

    def project():
        fetch("weight").wait()
        twin_own(twin).wait_recv()
        project_at(0)
        for step in range(steps):
            advance(QUARTERS * (step + 1) + 3)
            for way in range(2):
                if moved.get((way, step), -1) >= 0:
                    join(way, step)
                    moved[(way, step)] = -1
            for way in range(2):
                for place in order[way]:
                    if place[0] == step:
                        arrival(way, *place, "twin").wait_recv()
                if step < steps - 1 or way == 1:
                    project_at(-1 - step if way == 0 else 1 + step)

    def pair_at(i):
        offset = half + jnp.where(i % 2 == 1, -((i + 1) // 2), i // 2)
        return (me // 2 + offset) % pairs

    def squash():
        fetch("decay_low").wait()
        s["squashed"][...] = jnp.tanh(refs["decay_low"][...].astype(F32)).astype(BF16)
        fill_masks(s)
        for name in ("decay_up", "base", "rate_low", "rate_up", "key", "query"):
            fetch(name).wait()

    def in_groups(first, count, size, body):
        size = math.gcd(count, size)

        @pl.loop(0, count // size)
        def _(i):
            body([pair_at(first + i * size + j) for j in range(size)])

    def prepare_half(first):
        in_groups(first, half, 4, lambda chosen: prepare_group(chosen, refs, s))

    def refine_half(first):
        chosen = [pair_at(jnp.int32(first + j)) for j in range(half)]
        heads = [2 * pair + h for pair in chosen for h in range(2)]

        @pl.loop(0, 6)
        def _(level):
            refine_group(heads, level, s)

    def message_copy(head):
        return remote(
            s["message"].at[head],
            s["got"].at[me],
            s["message_send"].at[head],
            s["message_recv"].at[me],
            sp=head,
        )

    def send_messages(chosen):
        for pair in chosen:
            for h in range(2):
                head = 2 * pair + h

                @pl.when(head != me)
                def _():
                    message_copy(head).start()

    def solve_half(first):
        if first == 0:
            fetch("value").wait()
            fetch("gain").wait()
        size = math.gcd(half, 4)

        @pl.loop(0, half // size)
        def _(i):
            chosen = [pair_at(first + i * size + j) for j in range(size)]
            solve_group(chosen, refs, s)
            send_messages(chosen)

    low_half = lax.broadcasted_iota(jnp.int32, (HEAD, L), 1) < HEAD
    turn = lambda x: pltpu.roll(x, HEAD, 1)

    def unpack(n):
        both = s["got"][n, :HEAD].astype(F32)
        s["added"][n] = both
        s["moved"][n] = jnp.where(low_half, turn(both), 0.0).astype(BF16)
        parts = s["got"][n, HEAD:].astype(F32)
        s["kept"][n] = parts + turn(parts)

    def peer_at(j):
        offset = n_sp // 2 + jnp.where(j % 2 == 1, -((j + 1) // 2), j // 2)
        return (me + offset) % n_sp

    def unpack_all():
        s["got"][me] = s["message"][me]

        @pl.loop(0, n_sp - 1)
        def _(j):
            n = peer_at(j)
            remote(
                s["got"].at[n],
                s["got"].at[n],
                s["message_send"].at[n],
                s["message_recv"].at[n],
                sp=n,
            ).wait_recv()

        size = math.gcd(n_sp, 8)

        @pl.loop(0, n_sp // size)
        def _(i):
            for j in range(size):
                unpack(i * size + j)

    def state_copy(n):
        return remote(
            s["states"].at[n],
            s["starts"].at[me],
            s["state_send"].at[n],
            s["state_recv"].at[me],
            sp=n,
        )

    def on_state(state, x):
        high, low = split(x[HEAD:, :HEAD])
        left = rows(*split(state[:, :HEAD]))
        a = mm(left, high)
        return a[:HEAD] + a[HEAD:] + mm(left[:HEAD], low)

    def scan_all():
        spans = n_sp // SPAN
        row = lax.broadcasted_iota(jnp.int32, (2 * HEAD, L), 0)
        col = lax.broadcasted_iota(jnp.int32, (2 * HEAD, L), 1)
        start = (row == col + HEAD).astype(F32)
        xs = [start] * spans
        for j in range(SPAN):
            outs = []
            for g in range(spans):
                n = g * SPAN + j
                s["prefix"][n] = xs[g]
                outs.append(mm(rows(*split(xs[g][:, :HEAD])), s["moved"][n]))
            for g in range(spans):
                n = g * SPAN + j
                a = outs[g][: 2 * HEAD] + outs[g][2 * HEAD :]
                x = xs[g] * s["kept"][n][:1] - a
                xs[g] = rows(x[:HEAD] + s["added"][n], x[HEAD:])
        state = jnp.zeros((HEAD, HEAD), F32)
        for g in range(spans):
            s["entry"][g, :, :HEAD] = state
            if g + 1 < spans:
                state = on_state(state, xs[g]) + xs[g][:HEAD, :HEAD]

    def emit(n):
        x = s["prefix"][n]
        state = on_state(s["entry"][n // SPAN], x) + x[:HEAD, :HEAD]
        state = cols(state, state)
        s["states"][n] = jnp.where(
            low_half[: HEAD // 2], state[: HEAD // 2], state[HEAD // 2 :]
        ).astype(BF16)

    def emit_all():
        size = math.gcd(n_sp, 8)

        @pl.loop(0, n_sp // size)
        def _(i):
            for j in range(size):
                emit(peer_at(i * size + j))
            for j in range(size):
                n = peer_at(i * size + j)

                @pl.when(n != me)
                def _():
                    state_copy(n).start()

        s["starts"][me] = s["states"][me]

    def local_all():
        in_groups(0, pairs, 4, lambda chosen: local_group(chosen, refs, s))

    def wait_starts():
        @pl.loop(0, n_sp - 1)
        def _(j):
            n = peer_at(j)
            remote(
                s["starts"].at[n],
                s["starts"].at[n],
                s["state_send"].at[n],
                s["state_recv"].at[n],
                sp=n,
            ).wait_recv()

    def read_all():
        in_groups(0, pairs, 4, lambda chosen: read_group(chosen, refs, s))

    def drain():
        twin_own(me_dp).wait_send()
        for way in range(2):
            for place in order[way]:
                ring_copy(way, *place).wait_send()
                twin_copy(way, *place).wait_send()
                if place[1] == SHARED:
                    for k in range(1, along):
                        x_copy(way, place[0], k).wait_send()

        @pl.loop(1, n_sp)
        def _(j):
            n = (me + j) % n_sp
            message_copy(n).wait_send()
            state_copy(n).wait_send()

    phases = [
        ("greet", greet),
        ("fetch", fetch_all),
        ("met", met),
        ("weights", start_weights),
        ("squash", squash),
        ("prepare0", functools.partial(prepare_half, 0)),
        ("refine0", functools.partial(refine_half, 0)),
        ("solve0", functools.partial(solve_half, 0)),
        ("prepare1", functools.partial(prepare_half, half)),
        ("refine1", functools.partial(refine_half, half)),
        ("solve1", functools.partial(solve_half, half)),
        ("unpack", unpack_all),
        ("scan", scan_all),
        ("emit", emit_all),
        ("local", local_all),
        ("starts", wait_starts),
        ("read", read_all),
        ("project", project),
        ("drain", drain),
    ]
    for name, phase in phases:
        with jax.named_scope(name):
            phase()
        if name in schedule:
            with jax.named_scope("pass_" + name):
                advance(schedule[name])


SCHEDULE = {
    "prepare0": 1,
    "refine0": 2,
    "solve0": 3,
    "prepare1": 5,
    "refine1": 6,
    "solve1": 7,
    "unpack": 9,
    "emit": 10,
    "local": 11,
    "starts": 12,
}


def solution(mesh):
    n_sp, n_dp = mesh.shape["sp"], mesh.shape["dp"]

    def per_device(
        query_rows,
        key_rows,
        value_rows,
        decay_low,
        rate_low,
        decay_up,
        rate_up,
        decay_base,
        norm_gain,
        out_weight,
    ):
        width = query_rows.shape[2]
        vmem = pl.BlockSpec(memory_space=pltpu.VMEM)
        hbm = pl.BlockSpec(memory_space=pl.ANY)
        out = pl.pallas_call(
            functools.partial(
                whole_kernel, n_sp=n_sp, n_dp=n_dp, width=width, schedule=SCHEDULE
            ),
            out_shape=jax.ShapeDtypeStruct((L, n_dp * L), BF16),
            in_specs=[hbm] * len(INPUTS),
            out_specs=vmem,
            scratch_shapes=list(scratch(width, n_sp, n_dp).values()),
            compiler_params=pltpu.CompilerParams(
                collective_id=0, has_side_effects=True, vmem_limit_bytes=60 * 2**20
            ),
            name="mixer",
        )(
            query_rows[0],
            key_rows[0],
            value_rows[0],
            decay_low[0],
            rate_low[0],
            decay_up,
            rate_up,
            decay_base[None],
            norm_gain[None],
            out_weight,
        )
        return out[None]

    rows_spec = P("dp", "sp", None)
    return jax.shard_map(
        per_device,
        mesh=mesh,
        in_specs=(rows_spec,) * 5 + (P(), P(), P(), P(), P(None, "dp")),
        out_specs=rows_spec,
        check_vma=False,
    )
```

```python
import functools
import math

import jax
import jax.numpy as jnp
from jax import lax
from jax.experimental import pallas as pl
from jax.experimental.pallas import tpu as pltpu
from jax.sharding import PartitionSpec as P

HEAD = 64
L = 128
F32 = jnp.float32
BF16 = jnp.bfloat16
TAIL = 8
MSG = HEAD + TAIL
QUARTERS = 4
SPAN = 4
SHARED = 3
ALONG_X = 4


def split(x):
    high = x.astype(BF16)
    return high, (x - high.astype(F32)).astype(BF16)


def mm(a, b):
    return jnp.dot(a, b, preferred_element_type=F32)


def mm_t(a, b):
    return lax.dot_general(a, b, (((1,), (1,)), ((), ())), preferred_element_type=F32)


def t_mm(a, b):
    return lax.dot_general(a, b, (((0,), (0,)), ((), ())), preferred_element_type=F32)


def cols(*parts):
    return jnp.concatenate(parts, axis=1)


def rows(*parts):
    return jnp.concatenate(parts, axis=0)


def grid_index(n=L):
    return (
        lax.broadcasted_iota(jnp.int32, (n, n), 0),
        lax.broadcasted_iota(jnp.int32, (n, n), 1),
    )


def half_masks(dtype, width=L):
    lane = lax.broadcasted_iota(jnp.int32, (1, width), 1) % L
    return (lane < HEAD).astype(dtype), (lane >= HEAD).astype(dtype)


def prepare_group(chosen, refs, s):
    row, col = grid_index()
    first, second = half_masks(BF16)
    tri = (row >= col).astype(BF16)
    tri = cols(tri, tri)
    block = (row // HEAD == col // HEAD).astype(BF16)
    block = rows(block, block)
    held = []
    for pair in chosen:
        lanes = pl.ds(pl.multiple_of(pair * L, L), L)
        decay_pre = (
            refs["base"][:, lanes] + mm(s["squashed"][...], refs["decay_up"][:, lanes])
        ).astype(BF16)
        rate_pre = mm(refs["rate_low"][...], refs["rate_up"][:, lanes]).astype(BF16)
        log_decay = -math.exp(-0.5) / (1.0 + jnp.exp(-decay_pre.astype(F32)))
        rate = 1.0 / (1.0 + jnp.exp(-rate_pre.astype(F32)))
        running = mm(tri, rows(*split(log_decay)))
        key = refs["key"][:, lanes].astype(F32)
        total = mm(cols(*split(key * key)), block)
        held.append((pair, lanes, log_decay, rate, running, key, total))
    lefts = []
    for pair, lanes, log_decay, rate, running, key, total in held:
        before = running - log_decay
        centre = running[L // 2 : L // 2 + 1]
        final = running[L - 1 : L]
        query = refs["query"][:, lanes].astype(F32)
        unit = key * lax.rsqrt(1.0 + total)
        shrunk = jnp.exp(centre - running)
        read_mid = query * jnp.exp(running - centre)
        erase_from = unit * jnp.exp(before - centre)
        key_to = key * shrunk
        erase_to = unit * rate * shrunk
        up = jnp.exp(centre)
        down = jnp.exp(final - centre)
        s["read_start"][:, lanes] = read_mid * up
        s["erase_start"][:, lanes] = erase_from * up
        s["key_end"][:, lanes] = key_to * down
        s["erase_end"][:, lanes] = erase_to * down
        s["decay"][:, lanes] = jnp.exp(final)
        left = cols(*split(rows(erase_from, read_mid)))
        high, low = split(rows(key_to, erase_to))
        lefts.append((pair, left, high, low))
    for pair, left, high, low in lefts:
        for h, mask in enumerate((first, second)):
            a, b = high * mask, low * mask
            out = mm_t(left, cols(a, a)) + mm_t(left, cols(b, b))
            strict, within = s["strict"][...], s["within"][...]
            high_on, low_on = split(out[:L, :L] * strict)
            s["key_pairs"][pair, :, h * L : h * L + L] = high_on
            s["key_pairs"][pair, :, (2 + h) * L : (3 + h) * L] = low_on
            high_on, low_on = split(out[L:, :L] * within)
            s["read_keys"][pair, :, h * L : h * L + L] = high_on
            s["read_keys"][pair, :, (2 + h) * L : (3 + h) * L] = low_on
            high_on, low_on = split(out[L:, L:] * within)
            s["read_erase"][pair, :, h * L : h * L + L] = high_on
            s["read_erase"][pair, :, (2 + h) * L : (3 + h) * L] = low_on
            pairs = out[:L, L:] * strict
            high_on, low_on = split(pairs)
            head = 2 * pair + h
            s["lower"][head, :, :L] = high_on
            s["lower"][head, :, L:] = low_on
            s["inverse"][head] = s["eye"][...] - pairs * s["next_to"][...]


def times(left, right):
    a, b = split(right)
    row = cols(a, b)
    out = mm(left, rows(row, row))
    return out[:, :L] + out[:, L:]


def refine_group(chosen, level, s):
    held = [s["inverse"][head] for head in chosen]
    below = [
        times(s["lower"][head] * s["levels"][level], held[i]) for i, head in enumerate(chosen)
    ]
    for i, head in enumerate(chosen):
        s["inverse"][head] = held[i] - times(cols(*split(held[i])), below[i])


def fill_masks(s):
    row, col = grid_index()
    s["strict"][...] = (row > col).astype(F32)
    s["within"][...] = (row >= col).astype(F32)
    s["eye"][...] = (row == col).astype(F32)
    s["next_to"][...] = ((row // 2 == col // 2) & (row != col)).astype(F32)
    for level in range(1, 7):
        mask = (row >> (level + 1)) == (col >> (level + 1))
        mask = (mask & ((row >> level) != (col >> level))).astype(BF16)
        s["levels"][level - 1] = cols(mask, mask)


def on_pair(left, high, low):
    first, second = half_masks(BF16, 2 * L)
    high = rows(high * first, high * second)
    low = rows(low * first, low * second)
    return mm(left, rows(high, high)) + mm(left[:, : 2 * L], low)


def doubled(value):
    first, second = half_masks(BF16)
    both = rows(value * first, value * second)
    return rows(both, both)


def solve_group(chosen, refs, s):
    lanes_of = [pl.ds(pl.multiple_of(pair * L, L), L) for pair in chosen]
    carried = [
        mm(s["key_pairs"][pair], doubled(refs["value"][:, lanes]))
        for pair, lanes in zip(chosen, lanes_of)
    ]
    solved = []
    for pair, lanes, carry in zip(chosen, lanes_of, carried):
        d0, d1 = split(s["inverse"][2 * pair]), split(s["inverse"][2 * pair + 1])
        high, low = split(cols(s["erase_start"][:, lanes], carry))
        solved.append(split(on_pair(cols(d0[0], d1[0], d0[1], d1[1]), high, low)))
    low_half = lax.broadcasted_iota(jnp.int32, (HEAD, L), 1) < HEAD
    turn = lambda x: pltpu.roll(x, HEAD, 1)
    for pair, lanes, (high, low) in zip(chosen, lanes_of, solved):
        s["solved"][pair, :, : 2 * L] = high
        s["solved"][pair, :, 2 * L :] = low
        ends = cols(*split(s["erase_end"][:, lanes]))
        moved = t_mm(rows(high, low), rows(ends, ends))
        moved = moved[:, :L] + moved[:, L:]
        added = t_mm(refs["value"][:, lanes], cols(*split(s["key_end"][:, lanes])))
        added = added[:, :L] + added[:, L:] - moved[L:]
        moved = moved[:L]
        decay = jnp.broadcast_to(s["decay"][:, lanes], (TAIL, L))
        dh = decay.astype(BF16).astype(F32)
        dl = decay - dh
        s["message"][2 * pair, :HEAD] = jnp.where(
            low_half, added[:HEAD], turn(moved[:HEAD])
        ).astype(BF16)
        s["message"][2 * pair, HEAD:] = jnp.where(low_half[:TAIL], dh, turn(dl)).astype(BF16)
        s["message"][2 * pair + 1, :HEAD] = jnp.where(
            low_half, turn(added[HEAD:]), moved[HEAD:]
        ).astype(BF16)
        s["message"][2 * pair + 1, HEAD:] = jnp.where(low_half[:TAIL], turn(dh), dl).astype(BF16)


def local_group(chosen, refs, s):
    for pair in chosen:
        lanes = pl.ds(pl.multiple_of(pair * L, L), L)
        both = s["solved"][pair]
        on_erase = on_pair(s["read_erase"][pair], both[:, : 2 * L], both[:, 2 * L :])
        local = mm(s["read_keys"][pair], doubled(refs["value"][:, lanes]))
        s["read_state"][:, lanes] = s["read_start"][:, lanes] - on_erase[:, :L]
        s["local"][:, lanes] = local - on_erase[:, L:]


def read_group(chosen, refs, s):
    low_half = lax.broadcasted_iota(jnp.int32, (HEAD // 2, L), 1) < HEAD
    turn = lambda x: pltpu.roll(x, HEAD, 1)
    row, col = grid_index()
    block = (row // HEAD == col // HEAD).astype(BF16)
    block = rows(block, block)
    lanes_of = [pl.ds(pl.multiple_of(pair * L, L), L) for pair in chosen]
    readouts = []
    for pair, lanes in zip(chosen, lanes_of):
        a = s["starts"][2 * pair].astype(F32)
        b = s["starts"][2 * pair + 1].astype(F32)
        state = rows(
            jnp.where(low_half, a, 0.0),
            jnp.where(low_half, turn(a), 0.0),
            jnp.where(low_half, 0.0, turn(b)),
            jnp.where(low_half, 0.0, b),
        ).astype(BF16)
        readouts.append(
            mm_t(cols(*split(s["read_state"][:, lanes])), cols(state, state)) + s["local"][:, lanes]
        )
    centres = [x - mm(cols(*split(x)), block) * (1.0 / HEAD) for x in readouts]
    spreads = [mm(cols(*split(x * x)), block) * (1.0 / HEAD) for x in centres]
    for lanes, centred, variance in zip(lanes_of, centres, spreads):
        s["mix"][:, lanes] = (centred * lax.rsqrt(variance + 1.0) * refs["gain"][:, lanes]).astype(
            BF16
        )


def local_scratch(width):
    pairs = width // L
    wide = lambda: pltpu.VMEM((L, width), F32)
    return dict(
        squashed=pltpu.VMEM((L, L), BF16),
        read_start=wide(),
        erase_start=wide(),
        key_end=wide(),
        erase_end=wide(),
        decay=pltpu.VMEM((1, width), F32),
        key_pairs=pltpu.VMEM((pairs, L, 4 * L), BF16),
        read_keys=pltpu.VMEM((pairs, L, 4 * L), BF16),
        solved=pltpu.VMEM((pairs, L, 4 * L), BF16),
        strict=pltpu.VMEM((L, L), F32),
        within=pltpu.VMEM((L, L), F32),
        eye=pltpu.VMEM((L, L), F32),
        next_to=pltpu.VMEM((L, L), F32),
        levels=pltpu.VMEM((6, L, 2 * L), BF16),
        read_erase=pltpu.VMEM((pairs, L, 4 * L), BF16),
        lower=pltpu.VMEM((2 * pairs, L, 2 * L), BF16),
        inverse=pltpu.VMEM((2 * pairs, L, L), F32),
    )


INPUTS = (
    "query",
    "key",
    "value",
    "decay_low",
    "rate_low",
    "decay_up",
    "rate_up",
    "base",
    "gain",
    "weight",
)


def scratch(width, n_sp, n_dp):
    made = local_scratch(width)
    heads = width // HEAD
    chunks = n_dp // 4 * QUARTERS
    dma = pltpu.SemaphoreType.DMA
    made.update(
        read_state=pltpu.VMEM((L, width), F32),
        local=pltpu.VMEM((L, width), F32),
        message=pltpu.VMEM((heads, MSG, L), BF16),
        got=pltpu.VMEM((n_sp, MSG, L), BF16),
        added=pltpu.VMEM((n_sp, HEAD, L), F32),
        moved=pltpu.VMEM((n_sp, HEAD, L), BF16),
        kept=pltpu.VMEM((n_sp, 8, L), F32),
        prefix=pltpu.VMEM((n_sp, 2 * HEAD, L), F32),
        entry=pltpu.VMEM((n_sp // SPAN, HEAD, L), F32),
        states=pltpu.VMEM((n_sp, HEAD // 2, L), BF16),
        starts=pltpu.VMEM((heads, HEAD // 2, L), BF16),
        mix=pltpu.VMEM((L, width), BF16),
        weights=pltpu.VMEM((n_dp, width, L), BF16),
        query=pltpu.VMEM((L, width), BF16),
        key=pltpu.VMEM((L, width), BF16),
        value=pltpu.VMEM((L, width), BF16),
        decay_low=pltpu.VMEM((L, L), BF16),
        rate_low=pltpu.VMEM((L, L), BF16),
        decay_up=pltpu.VMEM((L, width), BF16),
        rate_up=pltpu.VMEM((L, width), BF16),
        base=pltpu.VMEM((1, width), F32),
        gain=pltpu.VMEM((1, width), F32),
        fetched=dma((len(INPUTS),)),
        x_send=dma,
        x_recv=dma((n_dp // 2,)),
        message_send=dma,
        message_recv=dma,
        state_send=dma,
        state_recv=dma,
        ring_send=dma,
        ring_recv=dma((2 * chunks,)),
        twin_send=dma,
        twin_recv=dma((n_dp // 2,)),
    )
    return made


MESH = pl.DeviceIdType.MESH


def remote(src, dst, send, recv, **where):
    return pltpu.make_async_remote_copy(
        src_ref=src, dst_ref=dst, send_sem=send, recv_sem=recv, device_id=where, device_id_type=MESH
    )


def whole_kernel(*args, n_sp, n_dp, width, schedule):
    given = dict(zip(INPUTS, args))
    out = args[len(INPUTS)]
    s = dict(zip(scratch(width, n_sp, n_dp), args[len(INPUTS) + 1 :]))
    refs = {name: s[name] for name in INPUTS if name != "weight"}
    pairs = width // L
    half = pairs // 2
    early = max(1, pairs // 4)
    me = lax.axis_index("sp")
    me_dp = lax.axis_index("dp")
    core, y, ring = me_dp % 2, me_dp // 2, n_dp // 2
    steps = ring // 2
    twin = y * 2 + 1 - core
    at = lambda offset, c: ((y + offset + ring) % ring) * 2 + c
    along = math.gcd(n_sp, ALONG_X)
    x = me % along
    barrier = pltpu.get_barrier_semaphore()

    def fetch(name):
        target = s["weights"].at[me_dp] if name == "weight" else s[name]
        return pltpu.make_async_copy(given[name], target, s["fetched"].at[INPUTS.index(name)])

    def fetch_all():
        for name in ("decay_low", "decay_up", "base", "rate_low", "rate_up", "key", "query"):
            fetch(name).start()
        for name in ("value", "gain", "weight"):
            fetch(name).start()

    def greet():
        @pl.loop(1, n_sp)
        def _(j):
            pl.semaphore_signal(
                barrier, inc=1, device_id={"sp": (me + j) % n_sp}, device_id_type=MESH
            )

        for peer in (twin, at(1, core), at(-1, core)):
            pl.semaphore_signal(barrier, inc=1, device_id={"dp": peer}, device_id_type=MESH)

    def met():
        pl.semaphore_wait(barrier, n_sp + 2)

    order = [
        [
            (step, quarter)
            for step in range(steps)
            for quarter in (
                ((SHARED, 0, 1, 2), (SHARED, 2, 0, 1))[way]
                if step < steps - 1
                else ((0, 1), (2, SHARED))[way]
            )
        ]
        for way in range(2)
    ]
    chunk = width // QUARTERS
    moved = {"chunks": 0}

    share = chunk // along

    def piece(ref, quarter):
        if quarter != SHARED:
            return ref.at[pl.ds(quarter * chunk, chunk)]
        return ref.at[pl.ds(pl.multiple_of(SHARED * chunk + x * share, share), share)]

    def whole_piece(ref, quarter):
        return ref.at[pl.ds(quarter * chunk, chunk)]

    def spot(way, step):
        return 2 * step + (way if step < steps - 1 else 0)

    def ring_copy(way, step, quarter):
        block = s["weights"].at[at(-step if way == 0 else step, core)]
        src = given["weight"] if step == 0 else block
        cut = piece if step < steps - 1 else whole_piece
        return remote(
            cut(src, quarter),
            cut(block, quarter),
            s["ring_send"],
            s["ring_recv"].at[(way * steps + step) * QUARTERS + quarter],
            dp=at(1 if way == 0 else -1, core),
        )

    def arrival(way, step, quarter):
        here = s["weights"].at[at(-1 - step if way == 0 else 1 + step, core)]
        here = (piece if step < steps - 1 else whole_piece)(here, quarter)
        recv = s["ring_recv"].at[(way * steps + step) * QUARTERS + quarter]
        return remote(here, here, s["ring_send"], recv, dp=at(1 if way == 0 else -1, core))

    def twin_copy(way, step, quarter):
        here = s["weights"].at[at(-1 - step if way == 0 else 1 + step, core)]
        here = whole_piece(here, quarter)
        return remote(here, here, s["twin_send"], s["twin_recv"].at[spot(way, step)], dp=twin)

    def twin_block(way, step):
        here = s["weights"].at[at(-1 - step if way == 0 else 1 + step, 1 - core)]
        return remote(here, here, s["twin_send"], s["twin_recv"].at[spot(way, step)], dp=twin)

    def twin_own(block):
        return remote(
            given["weight"],
            s["weights"].at[block],
            s["twin_send"],
            s["twin_recv"].at[2 * steps - 1],
            dp=twin,
        )

    def x_copy(way, step, k):
        here = piece(s["weights"].at[at(-1 - step if way == 0 else 1 + step, core)], SHARED)
        peer = me - x + (x + k) % along
        return remote(here, here, s["x_send"], s["x_recv"].at[spot(way, step)], sp=peer)

    def sent(kind, count):
        here = s["weights"].at[:, pl.ds(0, count // n_dp)]
        return remote(here, here, s[kind + "_send"], s["twin_recv"].at[0], dp=twin)

    def join(way, step):
        here = s["weights"].at[me_dp, pl.ds(0, share * (along - 1))]
        remote(here, here, s["x_send"], s["x_recv"].at[spot(way, step)], dp=twin).wait_recv()
        twin_copy(way, step, SHARED).start()
        if step == steps - 2 and (step + 1, SHARED) in order[way]:
            ring_copy(way, step + 1, SHARED).start()

    def advance(count):
        count = min(count, len(order[0]))
        for place in range(moved["chunks"], count):
            for way in range(2):
                step, quarter = order[way][place]
                arrival(way, step, quarter).wait_recv()
                parted = quarter == SHARED and step < steps - 1
                if (step + 1, quarter) in order[way] and not (parted and step == steps - 2):
                    ring_copy(way, step + 1, quarter).start()
                if parted:
                    for k in range(1, along):
                        x_copy(way, step, k).start()
                    moved[(way, step)] = place + 2
                else:
                    twin_copy(way, step, quarter).start()
            for way in range(2):
                for step in range(steps):
                    if moved.get((way, step)) == place:
                        join(way, step)
                        moved[(way, step)] = -1
        moved["chunks"] = max(count, moved["chunks"])

    def start_weights():
        for place in range(QUARTERS if steps > 1 else 2):
            for way in range(2):
                ring_copy(way, *order[way][place]).start()
        twin_own(me_dp).start()

    def project_at(offset):
        both = cols(s["weights"][at(offset, 0)], s["weights"][at(offset, 1)])
        where = pl.ds(pl.multiple_of(at(offset, 0) * L, 2 * L), 2 * L)
        out[:, where] = mm(s["mix"][...], both).astype(BF16)

    def project():
        fetch("weight").wait()
        twin_own(twin).wait_recv()
        project_at(0)
        for step in range(steps):
            advance(QUARTERS * (step + 1) + 3)
            for way in range(2):
                if moved.get((way, step), -1) >= 0:
                    join(way, step)
                    moved[(way, step)] = -1
            for way in range(2):
                if step < steps - 1 or way == 1:
                    twin_block(way, step).wait_recv()
                    project_at(-1 - step if way == 0 else 1 + step)

    def pair_at(i):
        offset = half + jnp.where(i % 2 == 1, -((i + 1) // 2), i // 2)
        return (me // 2 + offset) % pairs

    def squash():
        fetch("decay_low").wait()
        s["squashed"][...] = jnp.tanh(refs["decay_low"][...].astype(F32)).astype(BF16)
        fill_masks(s)
        for name in ("decay_up", "base", "rate_low", "rate_up", "key", "query"):
            fetch(name).wait()

    def in_groups(first, count, size, body):
        size = math.gcd(count, size)

        @pl.loop(0, count // size)
        def _(i):
            body([pair_at(first + i * size + j) for j in range(size)])

    def prepare_part(first, count):
        in_groups(first, count, 4, lambda chosen: prepare_group(chosen, refs, s))

    def refine_part(first, count, low, high):
        chosen = [pair_at(jnp.int32(first + j)) for j in range(count)]
        heads = [2 * pair + h for pair in chosen for h in range(2)]

        @pl.loop(low, high)
        def _(level):
            refine_group(heads, level, s)

    def message_copy(head):
        return remote(
            s["message"].at[head],
            s["got"].at[me],
            s["message_send"],
            s["message_recv"],
            sp=head,
        )

    def send_messages(chosen):
        for pair in chosen:
            for h in range(2):
                head = 2 * pair + h

                @pl.when(head != me)
                def _():
                    message_copy(head).start()

    def solve_part(first, count):
        if first == 0:
            fetch("value").wait()
            fetch("gain").wait()
        size = math.gcd(count, 4)

        @pl.loop(0, count // size)
        def _(i):
            chosen = [pair_at(first + i * size + j) for j in range(size)]
            solve_group(chosen, refs, s)
            send_messages(chosen)

    low_half = lax.broadcasted_iota(jnp.int32, (HEAD, L), 1) < HEAD
    turn = lambda x: pltpu.roll(x, HEAD, 1)

    def unpack(n):
        both = s["got"][n, :HEAD].astype(F32)
        s["added"][n] = both
        s["moved"][n] = jnp.where(low_half, turn(both), 0.0).astype(BF16)
        parts = s["got"][n, HEAD:].astype(F32)
        s["kept"][n] = parts + turn(parts)

    def peer_at(j):
        offset = n_sp // 2 + jnp.where(j % 2 == 1, -((j + 1) // 2), j // 2)
        return (me + offset) % n_sp

    def all_of(name, kind):
        rest = s[name].at[pl.ds(0, n_sp - 1)]
        return remote(rest, rest, s[kind + "_send"], s[kind + "_recv"], sp=(me + 1) % n_sp)

    def unpack_all():
        s["got"][me] = s["message"][me]

        all_of("got", "message").wait_recv()
        size = math.gcd(n_sp, 8)

        @pl.loop(0, n_sp // size)
        def _(i):
            for j in range(size):
                unpack(i * size + j)

    def state_copy(n):
        return remote(
            s["states"].at[n],
            s["starts"].at[me],
            s["state_send"],
            s["state_recv"],
            sp=n,
        )

    def on_state(state, x):
        high, low = split(x[HEAD:, :HEAD])
        left = rows(*split(state[:, :HEAD]))
        a = mm(left, high)
        return a[:HEAD] + a[HEAD:] + mm(left[:HEAD], low)

    def scan_all():
        spans = n_sp // SPAN
        row = lax.broadcasted_iota(jnp.int32, (2 * HEAD, L), 0)
        col = lax.broadcasted_iota(jnp.int32, (2 * HEAD, L), 1)
        start = (row == col + HEAD).astype(F32)
        xs = [start] * spans
        for j in range(SPAN):
            outs = []
            for g in range(spans):
                n = g * SPAN + j
                s["prefix"][n] = xs[g]
                outs.append(mm(rows(*split(xs[g][:, :HEAD])), s["moved"][n]))
            for g in range(spans):
                n = g * SPAN + j
                a = outs[g][: 2 * HEAD] + outs[g][2 * HEAD :]
                x = xs[g] * s["kept"][n][:1] - a
                xs[g] = rows(x[:HEAD] + s["added"][n], x[HEAD:])
        state = jnp.zeros((HEAD, HEAD), F32)
        for g in range(spans):
            s["entry"][g, :, :HEAD] = state
            if g + 1 < spans:
                state = on_state(state, xs[g]) + xs[g][:HEAD, :HEAD]

    def emit(n):
        x = s["prefix"][n]
        state = on_state(s["entry"][n // SPAN], x) + x[:HEAD, :HEAD]
        state = cols(state, state)
        s["states"][n] = jnp.where(
            low_half[: HEAD // 2], state[: HEAD // 2], state[HEAD // 2 :]
        ).astype(BF16)

    def emit_all():
        size = math.gcd(n_sp, 8)

        @pl.loop(0, n_sp // size)
        def _(i):
            for j in range(size):
                emit(peer_at(i * size + j))
            for j in range(size):
                n = peer_at(i * size + j)

                @pl.when(n != me)
                def _():
                    state_copy(n).start()

        s["starts"][me] = s["states"][me]

    def local_all():
        in_groups(0, pairs, 4, lambda chosen: local_group(chosen, refs, s))

        all_of("message", "message").wait_send()

    def wait_starts():
        all_of("starts", "state").wait_recv()

    def read_all():
        in_groups(0, pairs, 4, lambda chosen: read_group(chosen, refs, s))

    def drain():
        ringed = (steps - 1) * (3 * chunk + share) + 2 * chunk
        sent("ring", 2 * ringed).wait_send()
        sent("x", 2 * (steps - 1) * (along - 1) * share).wait_send()
        whole = s["weights"].at[pl.ds(0, n_dp // 2)]
        remote(whole, whole, s["twin_send"], s["twin_recv"].at[0], dp=twin).wait_send()
        all_of("states", "state").wait_send()

    phases = [
        ("greet", greet),
        ("fetch", fetch_all),
        ("met", met),
        ("weights", start_weights),
        ("squash", squash),
        ("prepare0", functools.partial(prepare_part, 0, early)),
        ("refine0a", functools.partial(refine_part, 0, early, 0, 3)),
        ("refine0b", functools.partial(refine_part, 0, early, 3, 6)),
        ("solve0", functools.partial(solve_part, 0, early)),
        ("prepare1", functools.partial(prepare_part, early, pairs - early)),
        ("refine1a", functools.partial(refine_part, early, pairs - early, 0, 3)),
        ("refine1b", functools.partial(refine_part, early, pairs - early, 3, 6)),
        ("solve1", functools.partial(solve_part, early, pairs - early)),
        ("unpack", unpack_all),
        ("scan", scan_all),
        ("emit", emit_all),
        ("local", local_all),
        ("starts", wait_starts),
        ("read", read_all),
        ("project", project),
        ("drain", drain),
    ]
    for name, phase in phases:
        with jax.named_scope(name):
            phase()
        if name in schedule:
            with jax.named_scope("pass_" + name):
                advance(schedule[name])


SCHEDULE = {
    "prepare1": 2,
    "refine1a": 3,
    "refine1b": 4,
    "solve1": 6,
    "unpack": 9,
    "emit": 10,
    "local": 11,
    "starts": 12,
    "read": 13,
}


def solution(mesh):
    n_sp, n_dp = mesh.shape["sp"], mesh.shape["dp"]

    def per_device(
        query_rows,
        key_rows,
        value_rows,
        decay_low,
        rate_low,
        decay_up,
        rate_up,
        decay_base,
        norm_gain,
        out_weight,
    ):
        width = query_rows.shape[2]
        vmem = pl.BlockSpec(memory_space=pltpu.VMEM)
        hbm = pl.BlockSpec(memory_space=pl.ANY)
        out = pl.pallas_call(
            functools.partial(
                whole_kernel, n_sp=n_sp, n_dp=n_dp, width=width, schedule=SCHEDULE
            ),
            out_shape=pltpu.VMEM((L, n_dp * L), BF16),
            in_specs=[hbm] * len(INPUTS),
            out_specs=vmem,
            scratch_shapes=list(scratch(width, n_sp, n_dp).values()),
            compiler_params=pltpu.CompilerParams(
                collective_id=0, has_side_effects=True, vmem_limit_bytes=60 * 2**20
            ),
            name="mixer",
        )(
            query_rows[0],
            key_rows[0],
            value_rows[0],
            decay_low[0],
            rate_low[0],
            decay_up,
            rate_up,
            decay_base[None],
            norm_gain[None],
            out_weight,
        )
        return out[None]

    rows_spec = P("dp", "sp", None)
    return jax.shard_map(
        per_device,
        mesh=mesh,
        in_specs=(rows_spec,) * 5 + (P(), P(), P(), P(), P(None, "dp")),
        out_specs=rows_spec,
        check_vma=False,
    )
```

```python
import functools
import math

import jax
import jax.numpy as jnp
from jax import lax
from jax.experimental import pallas as pl
from jax.experimental.pallas import tpu as pltpu
from jax.sharding import PartitionSpec as P

HEAD = 64
L = 128
F32 = jnp.float32
BF16 = jnp.bfloat16
TAIL = 8
MSG = HEAD + TAIL
QUARTERS = 4
SPAN = 4
SHARED = 3
ALONG_X = 4


def split(x):
    high = x.astype(BF16)
    return high, (x - high.astype(F32)).astype(BF16)


def mm(a, b):
    return jnp.dot(a, b, preferred_element_type=F32)


def mm_t(a, b):
    return lax.dot_general(a, b, (((1,), (1,)), ((), ())), preferred_element_type=F32)


def t_mm(a, b):
    return lax.dot_general(a, b, (((0,), (0,)), ((), ())), preferred_element_type=F32)


def cols(*parts):
    return jnp.concatenate(parts, axis=1)


def rows(*parts):
    return jnp.concatenate(parts, axis=0)


def grid_index(n=L):
    return (
        lax.broadcasted_iota(jnp.int32, (n, n), 0),
        lax.broadcasted_iota(jnp.int32, (n, n), 1),
    )


def half_masks(dtype, width=L):
    lane = lax.broadcasted_iota(jnp.int32, (1, width), 1) % L
    return (lane < HEAD).astype(dtype), (lane >= HEAD).astype(dtype)


def prepare_group(chosen, refs, s):
    row, col = grid_index()
    first, second = half_masks(BF16)
    tri = (row >= col).astype(BF16)
    tri = cols(tri, tri)
    block = (row // HEAD == col // HEAD).astype(BF16)
    block = rows(block, block)
    held = []
    for pair in chosen:
        lanes = pl.ds(pl.multiple_of(pair * L, L), L)
        decay_pre = (
            refs["base"][:, lanes] + mm(s["squashed"][...], refs["decay_up"][:, lanes])
        ).astype(BF16)
        rate_pre = mm(refs["rate_low"][...], refs["rate_up"][:, lanes]).astype(BF16)
        log_decay = -math.exp(-0.5) / (1.0 + jnp.exp(-decay_pre.astype(F32)))
        rate = 1.0 / (1.0 + jnp.exp(-rate_pre.astype(F32)))
        running = mm(tri, rows(*split(log_decay)))
        key = refs["key"][:, lanes].astype(F32)
        total = mm(cols(*split(key * key)), block)
        held.append((pair, lanes, log_decay, rate, running, key, total))
    lefts = []
    for pair, lanes, log_decay, rate, running, key, total in held:
        before = running - log_decay
        centre = running[L // 2 : L // 2 + 1]
        final = running[L - 1 : L]
        query = refs["query"][:, lanes].astype(F32)
        unit = key * lax.rsqrt(1.0 + total)
        shrunk = jnp.exp(centre - running)
        read_mid = query * jnp.exp(running - centre)
        erase_from = unit * jnp.exp(before - centre)
        key_to = key * shrunk
        erase_to = unit * rate * shrunk
        up = jnp.exp(centre)
        down = jnp.exp(final - centre)
        s["read_start"][:, lanes] = read_mid * up
        s["erase_start"][:, lanes] = erase_from * up
        s["key_end"][:, lanes] = key_to * down
        s["erase_end"][:, lanes] = erase_to * down
        s["decay"][:, lanes] = jnp.exp(final)
        left = cols(*split(rows(erase_from, read_mid)))
        high, low = split(rows(key_to, erase_to))
        lefts.append((pair, left, high, low))
    for pair, left, high, low in lefts:
        for h, mask in enumerate((first, second)):
            a, b = high * mask, low * mask
            out = mm_t(left, cols(a, a)) + mm_t(left, cols(b, b))
            strict, within = s["strict"][...], s["within"][...]
            high_on, low_on = split(out[:L, :L] * strict)
            s["key_pairs"][pair, :, h * L : h * L + L] = high_on
            s["key_pairs"][pair, :, (2 + h) * L : (3 + h) * L] = low_on
            high_on, low_on = split(out[L:, :L] * within)
            s["read_keys"][pair, :, h * L : h * L + L] = high_on
            s["read_keys"][pair, :, (2 + h) * L : (3 + h) * L] = low_on
            high_on, low_on = split(out[L:, L:] * within)
            s["read_erase"][pair, :, h * L : h * L + L] = high_on
            s["read_erase"][pair, :, (2 + h) * L : (3 + h) * L] = low_on
            pairs = out[:L, L:] * strict
            high_on, low_on = split(pairs)
            head = 2 * pair + h
            s["lower"][head, :, :L] = high_on
            s["lower"][head, :, L:] = low_on
            s["inverse"][head] = s["eye"][...] - pairs * s["next_to"][...]


def times(left, right):
    a, b = split(right)
    row = cols(a, b)
    out = mm(left, rows(row, row))
    return out[:, :L] + out[:, L:]


def refine_group(chosen, level, s):
    held = [s["inverse"][head] for head in chosen]
    below = [
        times(s["lower"][head] * s["levels"][level], held[i]) for i, head in enumerate(chosen)
    ]
    for i, head in enumerate(chosen):
        s["inverse"][head] = held[i] - times(cols(*split(held[i])), below[i])


def fill_masks(s):
    row, col = grid_index()
    s["strict"][...] = (row > col).astype(F32)
    s["within"][...] = (row >= col).astype(F32)
    s["eye"][...] = (row == col).astype(F32)
    s["next_to"][...] = ((row // 2 == col // 2) & (row != col)).astype(F32)
    for level in range(1, 7):
        mask = (row >> (level + 1)) == (col >> (level + 1))
        mask = (mask & ((row >> level) != (col >> level))).astype(BF16)
        s["levels"][level - 1] = cols(mask, mask)


def on_pair(left, high, low):
    first, second = half_masks(BF16, 2 * L)
    high = rows(high * first, high * second)
    low = rows(low * first, low * second)
    return mm(left, rows(high, high)) + mm(left[:, : 2 * L], low)


def doubled(value):
    first, second = half_masks(BF16)
    both = rows(value * first, value * second)
    return rows(both, both)


def solve_group(chosen, refs, s):
    lanes_of = [pl.ds(pl.multiple_of(pair * L, L), L) for pair in chosen]
    carried = [
        mm(s["key_pairs"][pair], doubled(refs["value"][:, lanes]))
        for pair, lanes in zip(chosen, lanes_of)
    ]
    solved = []
    for pair, lanes, carry in zip(chosen, lanes_of, carried):
        d0, d1 = split(s["inverse"][2 * pair]), split(s["inverse"][2 * pair + 1])
        high, low = split(cols(s["erase_start"][:, lanes], carry))
        solved.append(split(on_pair(cols(d0[0], d1[0], d0[1], d1[1]), high, low)))
    low_half = lax.broadcasted_iota(jnp.int32, (HEAD, L), 1) < HEAD
    turn = lambda x: pltpu.roll(x, HEAD, 1)
    for pair, lanes, (high, low) in zip(chosen, lanes_of, solved):
        s["solved"][pair, :, : 2 * L] = high
        s["solved"][pair, :, 2 * L :] = low
        ends = cols(*split(s["erase_end"][:, lanes]))
        moved = t_mm(rows(high, low), rows(ends, ends))
        moved = moved[:, :L] + moved[:, L:]
        added = t_mm(refs["value"][:, lanes], cols(*split(s["key_end"][:, lanes])))
        added = added[:, :L] + added[:, L:] - moved[L:]
        moved = moved[:L]
        decay = jnp.broadcast_to(s["decay"][:, lanes], (TAIL, L))
        dh = decay.astype(BF16).astype(F32)
        dl = decay - dh
        s["message"][2 * pair, :HEAD] = jnp.where(
            low_half, added[:HEAD], turn(moved[:HEAD])
        ).astype(BF16)
        s["message"][2 * pair, HEAD:] = jnp.where(low_half[:TAIL], dh, turn(dl)).astype(BF16)
        s["message"][2 * pair + 1, :HEAD] = jnp.where(
            low_half, turn(added[HEAD:]), moved[HEAD:]
        ).astype(BF16)
        s["message"][2 * pair + 1, HEAD:] = jnp.where(low_half[:TAIL], turn(dh), dl).astype(BF16)


def local_group(chosen, refs, s):
    for pair in chosen:
        lanes = pl.ds(pl.multiple_of(pair * L, L), L)
        both = s["solved"][pair]
        on_erase = on_pair(s["read_erase"][pair], both[:, : 2 * L], both[:, 2 * L :])
        local = mm(s["read_keys"][pair], doubled(refs["value"][:, lanes]))
        s["read_state"][:, lanes] = s["read_start"][:, lanes] - on_erase[:, :L]
        s["local"][:, lanes] = local - on_erase[:, L:]


def read_group(chosen, refs, s):
    low_half = lax.broadcasted_iota(jnp.int32, (HEAD // 2, L), 1) < HEAD
    turn = lambda x: pltpu.roll(x, HEAD, 1)
    row, col = grid_index()
    block = (row // HEAD == col // HEAD).astype(BF16)
    block = rows(block, block)
    lanes_of = [pl.ds(pl.multiple_of(pair * L, L), L) for pair in chosen]
    readouts = []
    for pair, lanes in zip(chosen, lanes_of):
        a = s["starts"][2 * pair].astype(F32)
        b = s["starts"][2 * pair + 1].astype(F32)
        state = rows(
            jnp.where(low_half, a, 0.0),
            jnp.where(low_half, turn(a), 0.0),
            jnp.where(low_half, 0.0, turn(b)),
            jnp.where(low_half, 0.0, b),
        ).astype(BF16)
        readouts.append(
            mm_t(cols(*split(s["read_state"][:, lanes])), cols(state, state)) + s["local"][:, lanes]
        )
    centres = [x - mm(cols(*split(x)), block) * (1.0 / HEAD) for x in readouts]
    spreads = [mm(cols(*split(x * x)), block) * (1.0 / HEAD) for x in centres]
    for lanes, centred, variance in zip(lanes_of, centres, spreads):
        s["mix"][:, lanes] = (centred * lax.rsqrt(variance + 1.0) * refs["gain"][:, lanes]).astype(
            BF16
        )


def local_scratch(width):
    pairs = width // L
    wide = lambda: pltpu.VMEM((L, width), F32)
    return dict(
        squashed=pltpu.VMEM((L, L), BF16),
        read_start=wide(),
        erase_start=wide(),
        key_end=wide(),
        erase_end=wide(),
        decay=pltpu.VMEM((1, width), F32),
        key_pairs=pltpu.VMEM((pairs, L, 4 * L), BF16),
        read_keys=pltpu.VMEM((pairs, L, 4 * L), BF16),
        solved=pltpu.VMEM((pairs, L, 4 * L), BF16),
        strict=pltpu.VMEM((L, L), F32),
        within=pltpu.VMEM((L, L), F32),
        eye=pltpu.VMEM((L, L), F32),
        next_to=pltpu.VMEM((L, L), F32),
        levels=pltpu.VMEM((6, L, 2 * L), BF16),
        read_erase=pltpu.VMEM((pairs, L, 4 * L), BF16),
        lower=pltpu.VMEM((2 * pairs, L, 2 * L), BF16),
        inverse=pltpu.VMEM((2 * pairs, L, L), F32),
    )


INPUTS = (
    "query",
    "key",
    "value",
    "decay_low",
    "rate_low",
    "decay_up",
    "rate_up",
    "base",
    "gain",
    "weight",
)


def scratch(width, n_sp, n_dp):
    made = local_scratch(width)
    heads = width // HEAD
    chunks = n_dp // 4 * QUARTERS
    dma = pltpu.SemaphoreType.DMA
    made.update(
        read_state=pltpu.VMEM((L, width), F32),
        local=pltpu.VMEM((L, width), F32),
        message=pltpu.VMEM((heads, MSG, L), BF16),
        got=pltpu.VMEM((n_sp, MSG, L), BF16),
        added=pltpu.VMEM((n_sp, HEAD, L), F32),
        moved=pltpu.VMEM((n_sp, HEAD, L), BF16),
        kept=pltpu.VMEM((n_sp, 8, L), F32),
        prefix=pltpu.VMEM((n_sp, 2 * HEAD, L), F32),
        entry=pltpu.VMEM((n_sp // SPAN, HEAD, L), F32),
        states=pltpu.VMEM((n_sp, HEAD // 2, L), BF16),
        starts=pltpu.VMEM((heads, HEAD // 2, L), BF16),
        mix=pltpu.VMEM((L, width), BF16),
        weights=pltpu.VMEM((n_dp, width, L), BF16),
        query=pltpu.VMEM((L, width), BF16),
        key=pltpu.VMEM((L, width), BF16),
        value=pltpu.VMEM((L, width), BF16),
        decay_low=pltpu.VMEM((L, L), BF16),
        rate_low=pltpu.VMEM((L, L), BF16),
        decay_up=pltpu.VMEM((L, width), BF16),
        rate_up=pltpu.VMEM((L, width), BF16),
        base=pltpu.VMEM((1, width), F32),
        gain=pltpu.VMEM((1, width), F32),
        fetched=dma((len(INPUTS),)),
        x_send=dma,
        x_recv=dma((n_dp // 2,)),
        message_send=dma,
        message_recv=dma,
        state_send=dma,
        state_recv=dma,
        ring_send=dma,
        ring_recv=dma((2 * chunks,)),
        twin_send=dma,
        twin_recv=dma((n_dp // 2,)),
    )
    return made


MESH = pl.DeviceIdType.MESH


def remote(src, dst, send, recv, **where):
    return pltpu.make_async_remote_copy(
        src_ref=src, dst_ref=dst, send_sem=send, recv_sem=recv, device_id=where, device_id_type=MESH
    )


def whole_kernel(*args, n_sp, n_dp, width, schedule):
    given = dict(zip(INPUTS, args))
    out = args[len(INPUTS)]
    s = dict(zip(scratch(width, n_sp, n_dp), args[len(INPUTS) + 1 :]))
    refs = {name: s[name] for name in INPUTS if name != "weight"}
    pairs = width // L
    half = pairs // 2
    early = half
    me = lax.axis_index("sp")
    me_dp = lax.axis_index("dp")
    core, y, ring = me_dp % 2, me_dp // 2, n_dp // 2
    steps = ring // 2
    twin = y * 2 + 1 - core
    at = lambda offset, c: ((y + offset + ring) % ring) * 2 + c
    along = math.gcd(n_sp, ALONG_X)
    x = me % along
    barrier = pltpu.get_barrier_semaphore()

    def fetch(name):
        target = s["weights"].at[me_dp] if name == "weight" else s[name]
        return pltpu.make_async_copy(given[name], target, s["fetched"].at[INPUTS.index(name)])

    def fetch_all():
        for name in ("decay_low", "decay_up", "base", "rate_low", "rate_up", "key", "query"):
            fetch(name).start()
        for name in ("value", "gain", "weight"):
            fetch(name).start()

    def greet():
        @pl.loop(1, n_sp)
        def _(j):
            pl.semaphore_signal(
                barrier, inc=1, device_id={"sp": (me + j) % n_sp}, device_id_type=MESH
            )

        for peer in (twin, at(1, core), at(-1, core)):
            pl.semaphore_signal(barrier, inc=1, device_id={"dp": peer}, device_id_type=MESH)

    def met():
        pl.semaphore_wait(barrier, n_sp + 2)

    order = [
        [
            (step, quarter)
            for step in range(steps)
            for quarter in (
                ((SHARED, 0, 1, 2), (SHARED, 2, 0, 1))[way]
                if step < steps - 1
                else ((0, 1), (2, SHARED))[way]
            )
        ]
        for way in range(2)
    ]
    chunk = width // QUARTERS
    moved = {"chunks": 0}

    share = chunk // along

    def piece(ref, quarter):
        if quarter != SHARED:
            return ref.at[pl.ds(quarter * chunk, chunk)]
        return ref.at[pl.ds(pl.multiple_of(SHARED * chunk + x * share, share), share)]

    def whole_piece(ref, quarter):
        return ref.at[pl.ds(quarter * chunk, chunk)]

    def spot(way, step):
        return 2 * step + (way if step < steps - 1 else 0)

    def ring_copy(way, step, quarter):
        block = s["weights"].at[at(-step if way == 0 else step, core)]
        src = given["weight"] if step == 0 else block
        cut = piece if step < steps - 1 else whole_piece
        return remote(
            cut(src, quarter),
            cut(block, quarter),
            s["ring_send"],
            s["ring_recv"].at[(way * steps + step) * QUARTERS + quarter],
            dp=at(1 if way == 0 else -1, core),
        )

    def arrival(way, step, quarter):
        here = s["weights"].at[at(-1 - step if way == 0 else 1 + step, core)]
        here = (piece if step < steps - 1 else whole_piece)(here, quarter)
        recv = s["ring_recv"].at[(way * steps + step) * QUARTERS + quarter]
        return remote(here, here, s["ring_send"], recv, dp=at(1 if way == 0 else -1, core))

    def twin_copy(way, step, quarter):
        here = s["weights"].at[at(-1 - step if way == 0 else 1 + step, core)]
        here = whole_piece(here, quarter)
        return remote(here, here, s["twin_send"], s["twin_recv"].at[spot(way, step)], dp=twin)

    def twin_block(way, step):
        here = s["weights"].at[at(-1 - step if way == 0 else 1 + step, 1 - core)]
        return remote(here, here, s["twin_send"], s["twin_recv"].at[spot(way, step)], dp=twin)

    def twin_own(block):
        return remote(
            given["weight"],
            s["weights"].at[block],
            s["twin_send"],
            s["twin_recv"].at[2 * steps - 1],
            dp=twin,
        )

    def x_copy(way, step, k):
        here = piece(s["weights"].at[at(-1 - step if way == 0 else 1 + step, core)], SHARED)
        peer = me - x + (x + k) % along
        return remote(here, here, s["x_send"], s["x_recv"].at[spot(way, step)], sp=peer)

    def sent(kind, count):
        here = s["weights"].at[:, pl.ds(0, count // n_dp)]
        return remote(here, here, s[kind + "_send"], s["twin_recv"].at[0], dp=twin)

    def join(way, step):
        here = s["weights"].at[me_dp, pl.ds(0, share * (along - 1))]
        remote(here, here, s["x_send"], s["x_recv"].at[spot(way, step)], dp=twin).wait_recv()
        twin_copy(way, step, SHARED).start()
        if step == steps - 2 and (step + 1, SHARED) in order[way]:
            ring_copy(way, step + 1, SHARED).start()

    def advance(count):
        count = min(count, len(order[0]))
        for place in range(moved["chunks"], count):
            for way in range(2):
                step, quarter = order[way][place]
                arrival(way, step, quarter).wait_recv()
                parted = quarter == SHARED and step < steps - 1
                if (step + 1, quarter) in order[way] and not (parted and step == steps - 2):
                    ring_copy(way, step + 1, quarter).start()
                if parted:
                    for k in range(1, along):
                        x_copy(way, step, k).start()
                    moved[(way, step)] = place + 2
                else:
                    twin_copy(way, step, quarter).start()
            for way in range(2):
                for step in range(steps):
                    if moved.get((way, step)) == place:
                        join(way, step)
                        moved[(way, step)] = -1
        moved["chunks"] = max(count, moved["chunks"])

    def start_weights():
        for place in range(QUARTERS if steps > 1 else 2):
            for way in range(2):
                ring_copy(way, *order[way][place]).start()
        twin_own(me_dp).start()

    def project_at(offset):
        both = cols(s["weights"][at(offset, 0)], s["weights"][at(offset, 1)])
        where = pl.ds(pl.multiple_of(at(offset, 0) * L, 2 * L), 2 * L)
        out[:, where] = mm(s["mix"][...], both).astype(BF16)

    def project():
        fetch("weight").wait()
        twin_own(twin).wait_recv()
        project_at(0)
        for step in range(steps):
            advance(QUARTERS * (step + 1) + 3)
            for way in range(2):
                if moved.get((way, step), -1) >= 0:
                    join(way, step)
                    moved[(way, step)] = -1
            for way in range(2):
                if step < steps - 1 or way == 1:
                    twin_block(way, step).wait_recv()
                    project_at(-1 - step if way == 0 else 1 + step)

    def pair_at(i):
        offset = half + jnp.where(i % 2 == 1, -((i + 1) // 2), i // 2)
        return (me // 2 + offset) % pairs

    def squash():
        fetch("decay_low").wait()
        s["squashed"][...] = jnp.tanh(refs["decay_low"][...].astype(F32)).astype(BF16)
        fill_masks(s)
        for name in ("decay_up", "base", "rate_low", "rate_up", "key", "query"):
            fetch(name).wait()

    def in_groups(first, count, size, body):
        size = math.gcd(count, size)

        @pl.loop(0, count // size)
        def _(i):
            body([pair_at(first + i * size + j) for j in range(size)])

    def prepare_part(first, count):
        in_groups(first, count, 4, lambda chosen: prepare_group(chosen, refs, s))

    def refine_part(first, count, low, high):
        chosen = [pair_at(jnp.int32(first + j)) for j in range(count)]
        heads = [2 * pair + h for pair in chosen for h in range(2)]

        @pl.loop(low, high)
        def _(level):
            refine_group(heads, level, s)

    def message_copy(head):
        return remote(
            s["message"].at[head],
            s["got"].at[me],
            s["message_send"],
            s["message_recv"],
            sp=head,
        )

    def send_messages(chosen):
        for pair in chosen:
            for h in range(2):
                head = 2 * pair + h

                @pl.when(head != me)
                def _():
                    message_copy(head).start()

    def solve_part(first, count):
        if first == 0:
            fetch("value").wait()
            fetch("gain").wait()
        size = math.gcd(count, 4)

        @pl.loop(0, count // size)
        def _(i):
            chosen = [pair_at(first + i * size + j) for j in range(size)]
            solve_group(chosen, refs, s)
            send_messages(chosen)

    low_half = lax.broadcasted_iota(jnp.int32, (HEAD, L), 1) < HEAD
    turn = lambda x: pltpu.roll(x, HEAD, 1)

    def unpack(n):
        both = s["got"][n, :HEAD].astype(F32)
        s["added"][n] = both
        s["moved"][n] = jnp.where(low_half, turn(both), 0.0).astype(BF16)
        parts = s["got"][n, HEAD:].astype(F32)
        s["kept"][n] = parts + turn(parts)

    def peer_at(j):
        offset = n_sp // 2 + jnp.where(j % 2 == 1, -((j + 1) // 2), j // 2)
        return (me + offset) % n_sp

    def all_of(name, kind):
        rest = s[name].at[pl.ds(0, n_sp - 1)]
        return remote(rest, rest, s[kind + "_send"], s[kind + "_recv"], sp=(me + 1) % n_sp)

    def unpack_all():
        s["got"][me] = s["message"][me]

        all_of("got", "message").wait_recv()
        size = math.gcd(n_sp, 8)

        @pl.loop(0, n_sp // size)
        def _(i):
            for j in range(size):
                unpack(i * size + j)

    def state_copy(n):
        return remote(
            s["states"].at[n],
            s["starts"].at[me],
            s["state_send"],
            s["state_recv"],
            sp=n,
        )

    def on_state(state, x):
        high, low = split(x[HEAD:, :HEAD])
        left = rows(*split(state[:, :HEAD]))
        a = mm(left, high)
        return a[:HEAD] + a[HEAD:] + mm(left[:HEAD], low)

    def scan_all():
        spans = n_sp // SPAN
        row = lax.broadcasted_iota(jnp.int32, (2 * HEAD, L), 0)
        col = lax.broadcasted_iota(jnp.int32, (2 * HEAD, L), 1)
        start = (row == col + HEAD).astype(F32)
        xs = [start] * spans
        for j in range(SPAN):
            outs = []
            for g in range(spans):
                n = g * SPAN + j
                s["prefix"][n] = xs[g]
                outs.append(mm(rows(*split(xs[g][:, :HEAD])), s["moved"][n]))
            for g in range(spans):
                n = g * SPAN + j
                a = outs[g][: 2 * HEAD] + outs[g][2 * HEAD :]
                x = xs[g] * s["kept"][n][:1] - a
                xs[g] = rows(x[:HEAD] + s["added"][n], x[HEAD:])
        state = jnp.zeros((HEAD, HEAD), F32)
        for g in range(spans):
            s["entry"][g, :, :HEAD] = state
            if g + 1 < spans:
                state = on_state(state, xs[g]) + xs[g][:HEAD, :HEAD]

    def emit(n):
        x = s["prefix"][n]
        state = on_state(s["entry"][n // SPAN], x) + x[:HEAD, :HEAD]
        state = cols(state, state)
        s["states"][n] = jnp.where(
            low_half[: HEAD // 2], state[: HEAD // 2], state[HEAD // 2 :]
        ).astype(BF16)

    def emit_all():
        size = math.gcd(n_sp, 8)

        @pl.loop(0, n_sp // size)
        def _(i):
            for j in range(size):
                emit(peer_at(i * size + j))
            for j in range(size):
                n = peer_at(i * size + j)

                @pl.when(n != me)
                def _():
                    state_copy(n).start()

        s["starts"][me] = s["states"][me]

    def local_all():
        in_groups(0, pairs, 4, lambda chosen: local_group(chosen, refs, s))

        all_of("message", "message").wait_send()

    def wait_starts():
        all_of("starts", "state").wait_recv()

    def read_all():
        in_groups(0, pairs, 4, lambda chosen: read_group(chosen, refs, s))

    def drain():
        ringed = (steps - 1) * (3 * chunk + share) + 2 * chunk
        sent("ring", 2 * ringed).wait_send()
        sent("x", 2 * (steps - 1) * (along - 1) * share).wait_send()
        whole = s["weights"].at[pl.ds(0, n_dp // 2)]
        remote(whole, whole, s["twin_send"], s["twin_recv"].at[0], dp=twin).wait_send()
        all_of("states", "state").wait_send()

    phases = [
        ("greet", greet),
        ("fetch", fetch_all),
        ("met", met),
        ("weights", start_weights),
        ("squash", squash),
        ("prepare0", functools.partial(prepare_part, 0, early)),
        ("refine0a", functools.partial(refine_part, 0, early, 0, 3)),
        ("refine0b", functools.partial(refine_part, 0, early, 3, 6)),
        ("solve0", functools.partial(solve_part, 0, early)),
        ("prepare1", functools.partial(prepare_part, early, pairs - early)),
        ("refine1a", functools.partial(refine_part, early, pairs - early, 0, 3)),
        ("refine1b", functools.partial(refine_part, early, pairs - early, 3, 6)),
        ("solve1", functools.partial(solve_part, early, pairs - early)),
        ("unpack", unpack_all),
        ("scan", scan_all),
        ("emit", emit_all),
        ("local", local_all),
        ("starts", wait_starts),
        ("read", read_all),
        ("project", project),
        ("drain", drain),
    ]
    for name, phase in phases:
        with jax.named_scope(name):
            phase()
        if name in schedule:
            with jax.named_scope("pass_" + name):
                advance(schedule[name])


SCHEDULE = {
    "solve0": 2,
    "prepare1": 3,
    "refine1b": 5,
    "solve1": 6,
    "unpack": 8,
    "scan": 9,
    "emit": 10,
    "local": 11,
    "starts": 12,
    "read": 13,
}


def solution(mesh):
    n_sp, n_dp = mesh.shape["sp"], mesh.shape["dp"]

    def per_device(
        query_rows,
        key_rows,
        value_rows,
        decay_low,
        rate_low,
        decay_up,
        rate_up,
        decay_base,
        norm_gain,
        out_weight,
    ):
        width = query_rows.shape[2]
        vmem = pl.BlockSpec(memory_space=pltpu.VMEM)
        hbm = pl.BlockSpec(memory_space=pl.ANY)
        out = pl.pallas_call(
            functools.partial(
                whole_kernel, n_sp=n_sp, n_dp=n_dp, width=width, schedule=SCHEDULE
            ),
            out_shape=pltpu.VMEM((L, n_dp * L), BF16),
            in_specs=[hbm] * len(INPUTS),
            out_specs=vmem,
            scratch_shapes=list(scratch(width, n_sp, n_dp).values()),
            compiler_params=pltpu.CompilerParams(
                collective_id=0, has_side_effects=True, vmem_limit_bytes=60 * 2**20
            ),
            name="mixer",
        )(
            query_rows[0],
            key_rows[0],
            value_rows[0],
            decay_low[0],
            rate_low[0],
            decay_up,
            rate_up,
            decay_base[None],
            norm_gain[None],
            out_weight,
        )
        return out[None]

    rows_spec = P("dp", "sp", None)
    return jax.shard_map(
        per_device,
        mesh=mesh,
        in_specs=(rows_spec,) * 5 + (P(), P(), P(), P(), P(None, "dp")),
        out_specs=rows_spec,
        check_vma=False,
    )
```
